128 devices in a mesh: ep: 32 (over z, y, core), tp: 4 (over x).
Axes of the slice: x: 4, y: 4, z: 4, core: 2. Of those that a mesh axis runs over, the one named last changes fastest.
Arguments:
- query_rows: bfloat16 [16384, 2048], P('ep', 'tp'), may hold values from -6 to 6
- key_rows: bfloat16 [16384, 512], P('ep', 'tp'), may hold values from -6 to 6
- value_rows: bfloat16 [16384, 512], P('ep', 'tp'), may hold values from -6 to 6
- query_gain: float32 [64], replicated, may hold values from 0.2 to 4.5
- key_gain: float32 [64], replicated, may hold values from 0.2 to 4.5
- sink_logit: float32 [32], P('tp'), may hold values from 2 to 6
- out_weight: bfloat16 [2048, 2048], P('tp'), may hold values from -0.125 to 0.125
- tokens: bfloat16 [16384, 2048], P('ep'), may hold values from -6 to 6
- norm_gain: float32 [2048], replicated, may hold values from 0.1 to 1.9
- expert_ids: int32 [16384, 2], P('ep'), may hold values from 0 to 127, all different within a row; in each aligned block of 128 rows (0 to 127, 128 to 255, ...) at most 4 rows name the same one
- route_weight: float32 [16384, 2], P('ep'), may hold values from 0.2 to 1
- gate_weight: bfloat16 [128, 2048, 1024], P('ep', None, 'tp'), may hold values from -0.125 to 0.125
- up_weight: bfloat16 [128, 2048, 1024], P('ep', None, 'tp'), may hold values from -0.125 to 0.125
- down_weight: bfloat16 [128, 1024, 2048], P('ep', 'tp'), may hold values from -0.1875 to 0.1875
- shared_gate: bfloat16 [2048, 1024], P(None, 'tp'), may hold values from -0.125 to 0.125
- shared_up: bfloat16 [2048, 1024], P(None, 'tp'), may hold values from -0.125 to 0.125
- shared_down: bfloat16 [1024, 2048], P('tp'), may hold values from -0.1875 to 0.1875
Outputs:
- mixer_out: bfloat16 [16384, 2048], P(('ep', 'tp'))
- expert_out: bfloat16 [16384, 2048], P(('ep', 'tp'))
The draws below stay inside these ranges and needn't reach their ends.
Inputs may be any that keep to these rules, and one draw needn't show every extreme that they name: `expert_ids`: each row names 2 different experts. In each aligned block of 128 rows no expert is named by more than 4 rows, a bound that some block reaches.
All inputs are finite; a program needn't handle non-finite values.
Results may differ from the reference program's by a relative error of at most 0.012.
The reference program's roundings to bfloat16 on the way count: a program that leaves them out, or rounds other values in their place, can miss the bound.
Values may be sent and summed in bfloat16 or wider, within the bound.
A program may use at most 128 MiB of HBM per device.

```python
import math
import jax
import jax.numpy as jnp
import numpy as np
from jax import lax

D = 2048
HEADS = 32
KV_HEADS = 8
HEAD_DIM = 64
FF = 1024
WINDOW = 128
BLOCK = 128
TOP_K = 2
B_ROWS = 128
EXPERTS = 128
CAP = 4
TOKENS_A = 16384
TOKENS_B = 16384
N_TP = 4


def attention_pair(key):
    base = jax.random.fold_in(key, 7001)
    first_key, second_key = jax.random.split(base)
    key_values = jax.random.normal(first_key, (TOKENS_A, KV_HEADS * HEAD_DIM), jnp.float32)
    query_values = jax.random.normal(second_key, (TOKENS_A, HEADS * HEAD_DIM), jnp.float32)
    return (jnp.clip(query_values, -6.0, 6.0), jnp.clip(key_values, -6.0, 6.0))


def gain_draw(key):
    return jnp.clip(1.0 + 0.18 * jax.random.normal(key, (HEAD_DIM,), jnp.float32), 0.2, 1.8)


def draw_query_rows(key, part):
    return attention_pair(key)[0].astype(jnp.bfloat16)


def draw_key_rows(key, part):
    return attention_pair(key)[1].astype(jnp.bfloat16)


def draw_query_gain(key, part):
    return gain_draw(jax.random.fold_in(key, 31))


def draw_key_gain(key, part):
    return gain_draw(jax.random.fold_in(key, 47))


def steps_of(stream_key, dims, cuts, low, high):
    factor_of = 1.0
    for axis_at, shards_of in cuts:
        steps = jax.random.uniform(jax.random.fold_in(jax.random.fold_in(stream_key, 6), axis_at), (shards_of,), jnp.float32, low / len(cuts), high / len(cuts))
        factor_of = factor_of * jnp.repeat(jnp.exp(steps), dims[axis_at] // shards_of).reshape((-1,) + (1,) * (len(dims) - 1 - axis_at))
    return factor_of


def assign_block(rng, own, number, rows, amount, top, limit, skew):
    order = jax.random.permutation(rng, amount)
    heavy_load, usual = load_shares(amount, rows * top, limit, skew, True), load_shares(amount, rows * top, limit, skew, False)
    places = jnp.arange(amount)

    def named(tallies, turn):
        used = int((tallies > 0).sum())
        fixed = max(1, used // 4)
        moved = fixed + (places - fixed + turn * (used - fixed)) % max(1, amount - fixed)
        return jnp.zeros((amount,), jnp.int32).at[order[jnp.where(places < fixed, places, moved)]].set(jnp.asarray(tallies, jnp.int32))

    tallies = jnp.where(number % 4 == 0, named(heavy_load, number // 4), named(usual, number - number // 4 - 1))
    mixed = jax.random.permutation(jax.random.fold_in(own, 3), amount)
    giver, taker = mixed[0:amount // 2 * 2:2], mixed[1:amount // 2 * 2:2]
    room = jnp.minimum(tallies[giver] - 1, limit - tallies[taker]) // 2
    room = jnp.where((giver == order[0]) | (taker == order[0]) | (tallies[taker] == 0), 0, jnp.maximum(room, 0))
    moved = jax.random.randint(jax.random.fold_in(own, 4), (amount // 2,), 0, 1 << 20) % (room + 1)
    tallies = tallies.at[giver].add(-moved).at[taker].add(moved)
    labels = jnp.searchsorted(jnp.cumsum(tallies), jnp.arange(rows * top), side="right").astype(jnp.int32)
    listing = labels.reshape(top, rows).T
    listing = listing[jax.random.permutation(jax.random.fold_in(own, 1), rows)]
    turn = jax.random.randint(jax.random.fold_in(own, 2), (rows, 1), 0, top)
    return jnp.take_along_axis(listing, (jnp.arange(top)[None, :] + turn) % top, axis=1)


def load_shares(count, total, limit, lean, full):
    weights = [(1 << 20) // math.isqrt(grade ** lean) + 1 for grade in range(1, count + 1)]
    largest = limit if full else min(limit, max(-(-total // count), total * weights[0] // sum(weights)))
    least = 1 if total - largest >= count - 1 else 0
    given, surplus = [largest] + [least] * (count - 1), total - largest - least * (count - 1)
    while surplus > 0:
        candidates = [i for i in range(1, count) if given[i] < largest] or [i for i in range(1, count) if given[i] < limit]
        pool, remaining = sum([weights[i] for i in candidates]), surplus
        for i in candidates:
            addition = min(limit - given[i], max(1, remaining * weights[i] // pool), surplus)
            given[i] = given[i] + addition
            surplus = surplus - addition
    return np.array(given)


def scatter_about(own_key, extent, width, bound, pieces=(), kind=jnp.bfloat16):
    result = width * jax.random.normal(own_key, extent, jnp.float32)
    if pieces:
        result = result * steps_of(own_key, extent, pieces, -0.22, 0.18)
    return jnp.clip(result, -bound, bound).astype(kind)


def setup_inputs(seed: int = 0) -> dict:
    key_list = jax.random.split(jax.random.key(seed), 18)
    query_rows = draw_query_rows(jax.random.fold_in(key_list[17], 71), 0)
    key_rows = draw_key_rows(jax.random.fold_in(key_list[17], 71), 0)
    value_rows = scatter_about(key_list[2], (TOKENS_A, KV_HEADS * HEAD_DIM), 1.0, 6.0, ((0, 32), (1, 4)))
    query_gain = draw_query_gain(jax.random.fold_in(key_list[17], 71), 0)
    key_gain = draw_key_gain(jax.random.fold_in(key_list[17], 71), 0)
    sink_logit = jnp.clip(2.0 + 4.0 * jax.random.uniform(key_list[5], (HEADS,), jnp.float32) ** steps_of(key_list[5], (HEADS,), ((0, 4),), -0.2, 0.2), 2.0, 6.0)
    out_weight = scatter_about(key_list[6], (HEADS * HEAD_DIM, D), (HEADS * HEAD_DIM) ** -0.5, 0.125, ((0, 4),))
    tokens = scatter_about(key_list[7], (TOKENS_B, D), 1.0, 6.0, ((0, 32),))
    norm_gain = jnp.clip(1.0 + 0.18 * jax.random.normal(key_list[8], (D,), jnp.float32), 0.1, 1.9)
    expert_ids_keys = jax.random.split(jax.random.fold_in(key_list[9], 1), TOKENS_B // B_ROWS)
    expert_ids_turns = jax.random.permutation(jax.random.fold_in(key_list[9], 3), TOKENS_B // B_ROWS)
    expert_ids = jax.vmap(lambda own, number: assign_block(jax.random.fold_in(key_list[9], 2), own, number, B_ROWS, EXPERTS, TOP_K, CAP, 1))(expert_ids_keys, expert_ids_turns).reshape((TOKENS_B, TOP_K))
    route_weight = jnp.clip(0.2 + 0.8 * jax.random.uniform(key_list[10], (TOKENS_B, TOP_K), jnp.float32) ** steps_of(key_list[10], (TOKENS_B, TOP_K), ((0, 32),), -0.2, 0.2), 0.2, 1.0)
    gate_weight = scatter_about(key_list[11], (EXPERTS, D, FF), D ** -0.5, 0.125, ((0, 32), (2, 4)))
    up_weight = scatter_about(key_list[12], (EXPERTS, D, FF), D ** -0.5, 0.125, ((0, 32), (2, 4)))
    down_weight = scatter_about(key_list[13], (EXPERTS, FF, D), FF ** -0.5, 0.1875, ((0, 32), (1, 4)))
    shared_gate = scatter_about(key_list[14], (D, FF), D ** -0.5, 0.125, ((1, 4),))
    shared_up = scatter_about(key_list[15], (D, FF), D ** -0.5, 0.125, ((1, 4),))
    shared_down = scatter_about(key_list[16], (FF, D), FF ** -0.5, 0.1875, ((0, 4),))
    return {"query_rows": query_rows, "key_rows": key_rows, "value_rows": value_rows, "query_gain": query_gain, "key_gain": key_gain, "sink_logit": sink_logit, "out_weight": out_weight, "tokens": tokens, "norm_gain": norm_gain, "expert_ids": expert_ids, "route_weight": route_weight, "gate_weight": gate_weight, "up_weight": up_weight, "down_weight": down_weight, "shared_gate": shared_gate, "shared_up": shared_up, "shared_down": shared_down}


epsilon = 1e-06
masked_score = -1e+30

def rms_scale(values, gain):
    widened = values.astype(jnp.float32)
    scaled = widened * lax.rsqrt(lax.optimization_barrier(jnp.mean(widened * widened, axis=-1, keepdims=True)) + epsilon)
    return (scaled * gain).astype(jnp.bfloat16)

def rounded_sum(hidden, weight):
    group_width = hidden.shape[-1] // N_TP
    running = jnp.zeros((hidden.shape[0], weight.shape[-1]), jnp.float32)
    for group_index in range(N_TP):
        lower = group_index * group_width
        partial_value = jnp.dot(hidden[:, lower:lower + group_width], weight[lower:lower + group_width], preferred_element_type=jnp.float32)
        running = running + lax.optimization_barrier(partial_value.astype(jnp.bfloat16)).astype(jnp.float32)
    return running.astype(jnp.bfloat16)

def expert_ffn(rows_in, gate_matrix, up_matrix, down_matrix):
    gate_part = jnp.dot(rows_in, gate_matrix, preferred_element_type=jnp.float32)
    up_part = jnp.dot(rows_in, up_matrix, preferred_element_type=jnp.float32)
    hidden = (jax.nn.silu(gate_part) * up_part).astype(jnp.bfloat16)
    return rounded_sum(hidden, down_matrix)

def window_mask(first_block, block_count):
    query_pos = jnp.arange(BLOCK)[:, None]
    key_pos = jnp.arange(2 * BLOCK)[None, :]
    inside = (key_pos <= query_pos + BLOCK) & (key_pos > query_pos + BLOCK - WINDOW)
    not_first = (first_block + jnp.arange(block_count))[:, None, None] > 0
    return inside[None] & (not_first | (key_pos[None] >= BLOCK))

def band_blocks(blocks_in):
    earlier = jnp.concatenate([jnp.zeros_like(blocks_in[:1]), blocks_in[:-1]], axis=0)
    return jnp.concatenate([earlier, blocks_in], axis=1)

def reference(query_rows, key_rows, value_rows, query_gain, key_gain, sink_logit, out_weight, tokens, norm_gain, expert_ids, route_weight, gate_weight, up_weight, down_weight, shared_gate, shared_up, shared_down):
    sequence_rows = query_rows.shape[0]
    blocks = sequence_rows // BLOCK
    group_size = HEADS // KV_HEADS
    query_normed = rms_scale(query_rows.reshape(blocks, BLOCK, KV_HEADS, group_size, HEAD_DIM), query_gain)
    key_normed = rms_scale(key_rows.reshape(blocks, BLOCK, KV_HEADS, HEAD_DIM), key_gain)
    key_band = band_blocks(key_normed)
    value_band = band_blocks(value_rows.reshape(blocks, BLOCK, KV_HEADS, HEAD_DIM))
    window = window_mask(0, blocks)
    score_scale = 1.0 / math.sqrt(HEAD_DIM)

    def one_head(inputs):
        query_head, key_head, value_head, sink_head = inputs
        scores = jnp.einsum('nqgd,nkd->gnqk', query_head.astype(jnp.float32), key_head.astype(jnp.float32)) * score_scale
        scores = jnp.where(window[None], scores, masked_score)
        sink_col = sink_head[:, None, None, None]
        row_max = jnp.maximum(lax.optimization_barrier(jnp.max(scores, axis=-1, keepdims=True)), sink_col)
        exp_scores = jnp.exp(scores - row_max)
        attn_probs = (exp_scores / (lax.optimization_barrier(jnp.sum(exp_scores, axis=-1, keepdims=True)) + jnp.exp(sink_col - row_max))).astype(jnp.bfloat16)
        return jnp.einsum('gnqk,nkd->nqgd', attn_probs.astype(jnp.float32), value_head.astype(jnp.float32)).astype(jnp.bfloat16)
    per_head = lax.map(one_head, (jnp.moveaxis(query_normed, 2, 0), jnp.moveaxis(key_band, 2, 0), jnp.moveaxis(value_band, 2, 0), sink_logit.reshape(KV_HEADS, group_size)))
    heads_out = jnp.moveaxis(per_head, 0, 2).reshape(sequence_rows, HEADS * HEAD_DIM)
    mixer_out = rounded_sum(heads_out, out_weight)
    normed = rms_scale(tokens, norm_gain)
    token_count = tokens.shape[0]
    flat_ids = expert_ids.reshape(-1).astype(jnp.int32)
    assign_count = flat_ids.shape[0]
    span_rows = 128
    sort_order = jnp.argsort(flat_ids, stable=True).astype(jnp.int32)
    sorted_ids = flat_ids[sort_order]
    counts = jnp.zeros((EXPERTS,), jnp.int32).at[flat_ids].add(1)
    starts = (jnp.cumsum(counts) - counts).astype(jnp.int32)
    padded = (counts + span_rows - 1) // span_rows * span_rows
    pad_ends = jnp.cumsum(padded).astype(jnp.int32)
    pad_starts = pad_ends - padded
    target = pad_starts[sorted_ids] + jnp.arange(assign_count, dtype=jnp.int32) - starts[sorted_ids]
    span_count = (assign_count + EXPERTS * (span_rows - 1) + span_rows - 1) // span_rows
    slot_assign = jnp.full((span_count * span_rows,), assign_count, jnp.int32).at[target].set(sort_order)
    span_expert = jnp.minimum(jnp.searchsorted(pad_ends, jnp.arange(span_count, dtype=jnp.int32) * span_rows, side='right'), EXPERTS - 1).astype(jnp.int32)
    padded_rows = jnp.concatenate([normed, jnp.zeros((1, D), jnp.bfloat16)], axis=0)

    def one_span(inputs):
        assigns, expert = inputs
        span_tokens = padded_rows[assigns // TOP_K]
        return expert_ffn(span_tokens, gate_weight[expert], up_weight[expert], down_weight[expert])
    span_out = lax.map(one_span, (slot_assign.reshape(span_count, span_rows), span_expert))
    per_assign = jnp.zeros((assign_count + 1, D), jnp.bfloat16).at[slot_assign].set(span_out.reshape(-1, D))
    routed = per_assign[:assign_count].reshape(token_count, TOP_K, D).astype(jnp.float32)
    shared_out = expert_ffn(normed, shared_gate, shared_up, shared_down)
    expert_out = (shared_out.astype(jnp.float32) + lax.optimization_barrier(jnp.sum(routed * route_weight[:, :, None], axis=1))).astype(jnp.bfloat16)
    return (mixer_out, expert_out)
```

```python
import jax
import jax.numpy as jnp
from jax import lax
from jax.experimental import pallas as pl
from jax.experimental.pallas import tpu as pltpu
from jax.sharding import Mesh
from jax.sharding import PartitionSpec as P

HEADS = 32
KV_HEADS = 8
HEAD_DIM = 64
BLOCK = 128
CAP = 4
N_TP = 4
NZ, NY, NC = 4, 4, 2
N_EP = NZ * NY * NC
EP = ("z", "y", "c")
EP_TP = ("z", "y", "c", "x")
D = 2048
ROWS = 512
FFS = 256
EXPERTS = 128
LOCAL = 4
COLS = D // N_TP
SLOTS = N_EP * 16
EPS = 1e-06
MASKED = -1e30
MESH_ID = pl.DeviceIdType.MESH
BF = jnp.bfloat16
F32 = jnp.float32

PAIRS = (
    (0, 1), (1, 0), (0, 3), (3, 0), (1, 2), (2, 1), (3, 2), (2, 3),
    (1, 1), (3, 3), (1, 3), (3, 1), (2, 0), (0, 2), (2, 2), (0, 0),
)
PEERS = tuple((dz, dy, dc) for dc in range(2) for dz, dy in PAIRS if (dz, dy, dc) != (0, 0, 0))


def dot(a, b):
    return jnp.dot(a, b, preferred_element_type=F32)


def layer_kernel(
    q_ref, k_ref, v_ref, qg_ref, kg_ref, sink_ref, gain_ref, ids_ref, rw_ref,
    tok_hbm, ow_hbm, wg_hbm, wu_hbm, wd_hbm, sg_hbm, su_hbm, sd_hbm,
    mix_out, exp_out,
    normed, ow, wg, wu, wd, sg, su, sd,
    slots, disp_send, disp_recv, rs_recv, ret_send, ret_recv,
    mix_send, mix_recv, sh_send, sh_recv, acc, fin_send, fin_recv,
    halo, kd, vd, heads,
    load_sem, dsend, drecv, rsend, rrecv, tsend, trecv,
    msend, mrecv, ssend, srecv, fsend, frecv, hsend, hrecv,
):
    z, y, c, x = (lax.axis_index(a) for a in EP_TP)
    me = (z * NY + y) * NC + c

    def ep_peer(off):
        dz, dy, dc = off
        pz, py, pc = lax.rem(z + dz, NZ), lax.rem(y + dy, NY), lax.rem(c + dc, NC)
        return (pz, py, pc, x), (pz * NY + py) * NC + pc

    def x_peer(d):
        px = lax.rem(x + d, N_TP)
        return (z, y, c, px), px

    barrier = pltpu.get_barrier_semaphore()
    for off in PEERS:
        pl.semaphore_signal(barrier, inc=1, device_id=ep_peer(off)[0], device_id_type=MESH_ID)
    for d in range(1, N_TP):
        pl.semaphore_signal(barrier, inc=1, device_id=x_peer(d)[0], device_id_type=MESH_ID)

    loads = [
        pltpu.make_async_copy(s, t, load_sem.at[i])
        for i, (s, t) in enumerate(
            [(tok_hbm, normed), (ow_hbm, ow), (sg_hbm, sg), (su_hbm, su), (sd_hbm, sd),
             (wg_hbm, wg), (wu_hbm, wu), (wd_hbm, wd)]
        )
    ]
    for cp in loads:
        cp.start()

    ids = ids_ref[...]
    expert = lax.broadcasted_iota(jnp.int32, (EXPERTS, ROWS), 0)
    first = (expert == ids[0:1, :]).astype(F32)
    second = (expert == ids[1:2, :]).astype(F32)
    s_row = lax.broadcasted_iota(jnp.int32, (ROWS, ROWS), 0)
    s_col = lax.broadcasted_iota(jnp.int32, (ROWS, ROWS), 1)
    earlier = ((s_row < s_col) & ((s_row >> 7) == (s_col >> 7))).astype(F32).astype(BF)
    seen = dot((first + second).astype(BF), earlier)
    rank_a = jnp.sum(first * seen, axis=0, keepdims=True)
    rank_b = jnp.sum(second * seen, axis=0, keepdims=True)
    place = (ids & 3) * SLOTS + (ids >> 2) * 16
    place = place + (lax.broadcasted_iota(jnp.int32, (2, ROWS), 1) >> 7) * CAP
    slots[0:1, :] = place[0:1, :].astype(F32) + rank_a
    slots[1:2, :] = place[1:2, :].astype(F32) + rank_b

    loads[0].wait()

    def norm_step(i, carry):
        rows = pl.ds(pl.multiple_of(i * 64, 64), 64)
        wide = normed[rows, :].astype(F32)
        scale = lax.rsqrt(jnp.mean(wide * wide, axis=-1, keepdims=True) + EPS)
        normed[rows, :] = ((wide * scale) * gain_ref[...]).astype(BF)
        return carry

    lax.fori_loop(0, ROWS // 64, norm_step, 0)

    mine = pl.ds(pl.multiple_of(me * 16, 16), 16)

    def slot_rows(j):
        index = lax.broadcasted_iota(jnp.int32, (SLOTS, ROWS), 0) + j * SLOTS
        return index.astype(F32)

    def send_chunk(j):
        for off in PEERS:
            dev, who = ep_peer(off)
            pltpu.make_async_remote_copy(
                src_ref=disp_send.at[j, pl.ds(pl.multiple_of(who * 16, 16), 16)],
                dst_ref=disp_recv.at[j, mine],
                send_sem=dsend.at[j], recv_sem=drecv.at[j],
                device_id=dev, device_id_type=MESH_ID,
            ).start()

    def whole_chunk(j):
        return pltpu.make_async_remote_copy(
            src_ref=disp_send.at[j, pl.ds(0, SLOTS - 16)],
            dst_ref=disp_recv.at[j, pl.ds(0, SLOTS - 16)],
            send_sem=dsend.at[j], recv_sem=drecv.at[j],
            device_id=ep_peer(PEERS[0])[0], device_id_type=MESH_ID,
        )

    def gather_step(j, carry):
        index = slot_rows(j)
        pick = (index == slots[0:1, :]) | (index == slots[1:2, :])
        pick = pick.astype(F32).astype(BF)
        for n in range(N_TP):
            cols = slice(n * COLS, (n + 1) * COLS)
            disp_send[j, :, cols] = dot(pick, normed[:, cols]).astype(BF)

        @pl.when(j == 0)
        def _():
            pl.semaphore_wait(barrier, len(PEERS) + N_TP - 1)

        @pl.when(j < 2)
        def _():
            send_chunk(j)

        disp_recv[j, mine, :] = disp_send[j, mine, :]
        return carry

    lax.fori_loop(0, LOCAL, gather_step, 0)

    nxt = lax.rem(me + 1, N_EP)
    nxt_dev = (nxt // (NY * NC), lax.rem(nxt // NC, NY), lax.rem(nxt, NC), x)
    halos = [
        pltpu.make_async_remote_copy(
            src_ref=ref.at[pl.ds(ROWS - BLOCK, BLOCK)], dst_ref=halo.at[i],
            send_sem=hsend.at[i], recv_sem=hrecv.at[i],
            device_id=nxt_dev, device_id_type=MESH_ID,
        )
        for i, ref in enumerate((k_ref, v_ref))
    ]
    for cp in halos:
        cp.start()

    loads[2].wait()
    loads[3].wait()
    loads[4].wait()
    gate = dot(normed[...], sg[...])
    up = dot(normed[...], su[...])
    hidden = (gate / (1.0 + jnp.exp(-gate)) * up).astype(BF)
    for n in range(N_TP):
        cols = slice(n * COLS, (n + 1) * COLS)
        sh_send[:, cols] = dot(hidden, sd[:, cols]).astype(BF)

    def col_block(px):
        return pl.ds(pl.multiple_of(px * COLS, COLS), COLS)

    def shared_copies():
        out = []
        for d in range(1, N_TP):
            dev, px = x_peer(d)
            out.append(pltpu.make_async_remote_copy(
                src_ref=sh_send.at[:, col_block(px)], dst_ref=sh_recv.at[d - 1],
                send_sem=ssend.at[d - 1], recv_sem=srecv.at[d - 1],
                device_id=dev, device_id_type=MESH_ID,
            ))
        return out

    lane = lax.broadcasted_iota(jnp.int32, (1, 128), 1)
    low = lane < HEAD_DIM
    half_a = lax.broadcasted_iota(jnp.int32, (128, 128), 0) >> 6
    half_b = lax.broadcasted_iota(jnp.int32, (128, 128), 1) >> 6
    same_half = (half_a == half_b).astype(F32).astype(BF)

    def head_norm(rows_in, gain):
        wide = rows_in.astype(F32)
        square = wide * wide
        top = square.astype(BF)
        rest = (square - top.astype(F32)).astype(BF)
        total = dot(top, same_half) + dot(rest, same_half)
        scale = lax.rsqrt(total * (1.0 / HEAD_DIM) + EPS)
        return ((wide * scale) * gain).astype(BF)

    def both_halves(rows_in, dst, rows):
        wide = rows_in.astype(F32)
        turned = pltpu.roll(wide, HEAD_DIM, 1)
        dst[0, rows, :] = jnp.where(low, wide, turned).astype(BF)
        dst[1, rows, :] = jnp.where(low, turned, wide).astype(BF)

    own_rows = slice(BLOCK, BLOCK + ROWS)
    both_halves(head_norm(k_ref[...], kg_ref[...]), kd, own_rows)
    both_halves(v_ref[...], vd, own_rows)
    for cp in halos:
        cp.wait()
    both_halves(head_norm(halo[0], kg_ref[...]), kd, slice(0, BLOCK))
    both_halves(halo[1], vd, slice(0, BLOCK))
    query_pos = lax.broadcasted_iota(jnp.int32, (BLOCK, 2 * BLOCK), 0)
    key_pos = lax.broadcasted_iota(jnp.int32, (BLOCK, 2 * BLOCK), 1)

    def attend(n, carry):
        rows = pl.ds(pl.multiple_of(n * BLOCK, BLOCK), BLOCK)
        band = pl.ds(pl.multiple_of(n * BLOCK, BLOCK), 2 * BLOCK)
        floor = jnp.where(me * 4 + n == 0, BLOCK, 0)
        inside = (key_pos <= query_pos + BLOCK) & (key_pos > query_pos) & (key_pos >= floor)
        for kv in range(2):
            parts = []
            for b in range(2):
                cols = slice((kv * 2 + b) * 128, (kv * 2 + b + 1) * 128)
                qn = head_norm(q_ref[rows, cols], qg_ref[...]).astype(F32)
                parts.append(jnp.where(low, qn, 0.0).astype(BF))
                parts.append(jnp.where(low, 0.0, qn).astype(BF))
            stacked = jnp.concatenate(parts, axis=0)
            scores = lax.dot_general(
                stacked, kd[kv, band, :], (((1,), (1,)), ((), ())), preferred_element_type=F32
            ) * 0.125
            probs = []
            for g in range(4):
                sink = sink_ref[0, kv * 4 + g]
                part = jnp.where(inside, scores[g * BLOCK:(g + 1) * BLOCK], MASKED)
                top = jnp.maximum(jnp.max(part, axis=-1, keepdims=True), sink)
                ex = jnp.exp(part - top)
                den = jnp.sum(ex, axis=-1, keepdims=True) + jnp.exp(sink - top)
                probs.append((ex * (1.0 / den)).astype(BF))
            mixed = dot(jnp.concatenate(probs, axis=0), vd[kv, band, :])
            for b in range(2):
                lo = mixed[(2 * b) * BLOCK:(2 * b + 1) * BLOCK]
                hi = mixed[(2 * b + 1) * BLOCK:(2 * b + 2) * BLOCK]
                cols = slice((kv * 2 + b) * 128, (kv * 2 + b + 1) * 128)
                heads[rows, cols] = jnp.where(low, lo, hi).astype(BF)
        return carry

    for cp in shared_copies():
        cp.start()

    lax.fori_loop(0, ROWS // BLOCK, attend, 0)
    loads[1].wait()
    for n in range(N_TP):
        cols = slice(n * COLS, (n + 1) * COLS)
        mix_send[:, cols] = dot(heads[...], ow[:, cols]).astype(BF)

    def quarter(px):
        return pl.ds(pl.multiple_of(px * BLOCK, BLOCK), BLOCK)

    def mixer_copies():
        out = []
        for d in range(1, N_TP):
            dev, px = x_peer(d)
            out.append(pltpu.make_async_remote_copy(
                src_ref=mix_send.at[quarter(px)], dst_ref=mix_recv.at[d - 1],
                send_sem=msend.at[d - 1], recv_sem=mrecv.at[d - 1],
                device_id=dev, device_id_type=MESH_ID,
            ))
        return out

    for cp in mixer_copies():
        cp.start()

    loads[5].wait()
    loads[6].wait()
    loads[7].wait()

    def rs_copies(j):
        out = []
        for d in range(1, N_TP):
            dev, px = x_peer(d)
            out.append(pltpu.make_async_remote_copy(
                src_ref=disp_send.at[j, :, col_block(px)], dst_ref=rs_recv.at[j, d - 1],
                send_sem=rsend.at[j, d - 1], recv_sem=rrecv.at[j, d - 1],
                device_id=dev, device_id_type=MESH_ID,
            ))
        return out

    def whole_return(j):
        return pltpu.make_async_remote_copy(
            src_ref=ret_send.at[j, pl.ds(0, SLOTS - 16)],
            dst_ref=ret_recv.at[j, pl.ds(0, SLOTS - 16)],
            send_sem=tsend.at[j], recv_sem=trecv.at[j],
            device_id=ep_peer(PEERS[0])[0], device_id_type=MESH_ID,
        )

    def step(i, carry):
        @pl.when(i < LOCAL)
        def _():
            whole_chunk(i).wait()

            @pl.when(i < 2)
            def _():
                send_chunk(i + 2)

            gate = dot(disp_recv[i], wg[i])
            up = dot(disp_recv[i], wu[i])
            hidden = (gate / (1.0 + jnp.exp(-gate)) * up).astype(BF)
            for n in range(N_TP):
                cols = slice(n * COLS, (n + 1) * COLS)
                disp_send[i, :, cols] = dot(hidden, wd[i, :, cols]).astype(BF)
            for cp in rs_copies(i):
                cp.start()

        @pl.when(i == LOCAL)
        def _():
            for cp in mixer_copies():
                cp.wait()
            total = mix_send[quarter(x), :].astype(F32)
            for d in range(N_TP - 1):
                total = total + mix_recv[d].astype(F32)
            mix_out[...] = total.astype(BF)

        @pl.when((i >= 1) & (i <= LOCAL))
        def _():
            j = i - 1
            for cp in rs_copies(j):
                cp.wait()
            total = disp_send[j, :, col_block(x)].astype(F32)
            for d in range(N_TP - 1):
                total = total + rs_recv[j, d].astype(F32)
            ret_send[j] = total.astype(BF)
            for off in PEERS:
                dev, who = ep_peer(off)
                pltpu.make_async_remote_copy(
                    src_ref=ret_send.at[j, pl.ds(pl.multiple_of(who * 16, 16), 16)],
                    dst_ref=ret_recv.at[j, mine],
                    send_sem=tsend.at[j], recv_sem=trecv.at[j],
                    device_id=dev, device_id_type=MESH_ID,
                ).start()
            ret_recv[j, mine, :] = ret_send[j, mine, :]

        @pl.when(i == 2)
        def _():
            for cp in shared_copies():
                cp.wait()
            total = sh_send[:, col_block(x)].astype(F32)
            for d in range(N_TP - 1):
                total = total + sh_recv[d].astype(F32)
            acc[...] = total.astype(BF).astype(F32)

        @pl.when(i >= 2)
        def _():
            j = i - 2
            whole_return(j).wait()
            index = slot_rows(j)
            weight = jnp.where(index == slots[0:1, :], rw_ref[0:1, :], 0.0)
            weight = weight + jnp.where(index == slots[1:2, :], rw_ref[1:2, :], 0.0)
            main = weight.astype(BF)
            rest = (weight - main.astype(F32)).astype(BF)
            dims = (((0,), (0,)), ((), ()))
            back = ret_recv[j]
            acc[...] += lax.dot_general(
                main, back, dims, preferred_element_type=F32
            ) + lax.dot_general(rest, back, dims, preferred_element_type=F32)

        return carry

    lax.fori_loop(0, LOCAL + 2, step, 0)

    fin_send[...] = acc[...].astype(BF)
    finals = []
    for d in range(1, N_TP):
        dev, px = x_peer(d)
        finals.append(pltpu.make_async_remote_copy(
            src_ref=fin_send.at[quarter(px)], dst_ref=fin_recv.at[d - 1],
            send_sem=fsend.at[d - 1], recv_sem=frecv.at[d - 1],
            device_id=dev, device_id_type=MESH_ID,
        ))
    for cp in finals:
        cp.start()
    exp_out[:, col_block(x)] = fin_send[quarter(x), :]
    for d, cp in enumerate(finals):
        cp.wait()
        exp_out[:, col_block(lax.rem(x + N_TP - 1 - d, N_TP))] = fin_recv[d]


def shards(
    query_rows, key_rows, value_rows, query_gain, key_gain, sink_logit, out_weight, tokens,
    norm_gain, expert_ids, route_weight, gate_weight, up_weight, down_weight,
    shared_gate, shared_up, shared_down,
):
    vmem = pl.BlockSpec(memory_space=pltpu.VMEM)
    hbm = pl.BlockSpec(memory_space=pl.ANY)
    smem = pl.BlockSpec(memory_space=pltpu.SMEM)
    dma = pltpu.SemaphoreType.DMA
    out = jax.ShapeDtypeStruct((BLOCK, D), BF)
    return pl.pallas_call(
        layer_kernel,
        out_shape=(out, out),
        in_specs=[vmem] * 5 + [smem] + [vmem] * 3 + [hbm] * 8,
        out_specs=(vmem, vmem),
        scratch_shapes=[
            pltpu.VMEM((ROWS, D), BF),
            pltpu.VMEM((ROWS, D), BF),
            pltpu.VMEM((LOCAL, D, FFS), BF),
            pltpu.VMEM((LOCAL, D, FFS), BF),
            pltpu.VMEM((LOCAL, FFS, D), BF),
            pltpu.VMEM((D, FFS), BF),
            pltpu.VMEM((D, FFS), BF),
            pltpu.VMEM((FFS, D), BF),
            pltpu.VMEM((2, ROWS), F32),
            pltpu.VMEM((LOCAL, SLOTS, D), BF),
            pltpu.VMEM((LOCAL, SLOTS, D), BF),
            pltpu.VMEM((LOCAL, N_TP - 1, SLOTS, COLS), BF),
            pltpu.VMEM((LOCAL, SLOTS, COLS), BF),
            pltpu.VMEM((LOCAL, SLOTS, COLS), BF),
            pltpu.VMEM((ROWS, D), BF),
            pltpu.VMEM((N_TP - 1, BLOCK, D), BF),
            pltpu.VMEM((ROWS, D), BF),
            pltpu.VMEM((N_TP - 1, ROWS, COLS), BF),
            pltpu.VMEM((ROWS, COLS), F32),
            pltpu.VMEM((ROWS, COLS), BF),
            pltpu.VMEM((N_TP - 1, BLOCK, COLS), BF),
            pltpu.VMEM((2, BLOCK, 128), BF),
            pltpu.VMEM((2, BLOCK + ROWS, 128), BF),
            pltpu.VMEM((2, BLOCK + ROWS, 128), BF),
            pltpu.VMEM((ROWS, 512), BF),
            dma((8,)),
            dma((LOCAL,)), dma((LOCAL,)),
            dma((LOCAL, N_TP - 1)), dma((LOCAL, N_TP - 1)),
            dma((LOCAL,)), dma((LOCAL,)),
            dma((N_TP - 1,)), dma((N_TP - 1,)),
            dma((N_TP - 1,)), dma((N_TP - 1,)),
            dma((N_TP - 1,)), dma((N_TP - 1,)),
            dma((2,)), dma((2,)),
        ],
        compiler_params=pltpu.CompilerParams(
            collective_id=0, has_side_effects=True, vmem_limit_bytes=67000000
        ),
        name="layer",
    )(
        query_rows, key_rows, value_rows,
        jnp.tile(query_gain, 2)[None], jnp.tile(key_gain, 2)[None],
        sink_logit[None], norm_gain[None], expert_ids.T, route_weight.T,
        tokens, out_weight, gate_weight, up_weight, down_weight,
        shared_gate, shared_up, shared_down,
    )


def solution(mesh):
    split = Mesh(mesh.devices.reshape(NZ, NY, NC, mesh.shape["tp"]), EP_TP)
    return jax.shard_map(
        shards,
        mesh=split,
        in_specs=(
            P(EP, "x"), P(EP, "x"), P(EP, "x"), P(), P(), P("x"), P("x", None),
            P(EP, None), P(), P(EP, None), P(EP, None),
            P(EP, None, "x"), P(EP, None, "x"), P(EP, "x", None),
            P(None, "x"), P(None, "x"), P("x", None),
        ),
        out_specs=(P(EP_TP, None), P(EP_TP, None)),
        check_vma=False,
    )
```

```python
import jax
import jax.numpy as jnp
from jax import lax
from jax.experimental import pallas as pl
from jax.experimental.pallas import tpu as pltpu
from jax.sharding import Mesh
from jax.sharding import PartitionSpec as P

HEADS = 32
KV_HEADS = 8
HEAD_DIM = 64
BLOCK = 128
CAP = 4
N_TP = 4
NZ, NY, NC = 4, 4, 2
N_EP = NZ * NY * NC
EP = ("z", "y", "c")
EP_TP = ("z", "y", "c", "x")
D = 2048
ROWS = 512
FFS = 256
EXPERTS = 128
LOCAL = 4
COLS = D // N_TP
SLOTS = N_EP * 16
EPS = 1e-06
MASKED = -1e30
MESH_ID = pl.DeviceIdType.MESH
BF = jnp.bfloat16
F32 = jnp.float32

ORDER = tuple(((k + k // NY) % NZ) * NY + k % NY for k in range(NZ * NY))
HALVES = tuple(tuple(dc * NZ * NY + o for o in ORDER if (dc, o) != (0, 0)) for dc in range(NC))
PEERS = HALVES[0] + HALVES[1]
HALF = SLOTS // 2


def dot(a, b):
    return jnp.dot(a, b, preferred_element_type=F32)


def layer_kernel(
    q_ref, k_ref, v_ref, qg_ref, kg_ref, sink_ref, gain_ref, ids_ref, rw_ref,
    tok_hbm, ow_hbm, wg_hbm, wu_hbm, wd_hbm, sg_hbm, su_hbm, sd_hbm,
    mix_out, exp_out,
    normed, ow, wg, wu, wd, sg, su, sd,
    slots, disp_send, disp_recv, rs_relay, rs_side, ret_send, ret_recv,
    mix_send, mix_relay, mix_side, sh_send, sh_relay, sh_side, acc, fin_send, fin_recv,
    halo, kd, vd, heads,
    load_sem, dsend, drecv, xsend, xrecv, tsend, trecv, fsend, frecv, hsend, hrecv,
):
    z, y, c, x = (lax.axis_index(a) for a in EP_TP)
    me = (z * NY + y) * NC + c

    def ep_peer(slot, sign=1):
        dc, dz, dy = slot // (NZ * NY), slot // NY % NZ, slot % NY
        return (
            lax.rem(z + (dz * sign) % NZ, NZ), lax.rem(y + (dy * sign) % NY, NY),
            lax.rem(c + dc, NC), x,
        )

    def x_peer(d):
        return (z, y, c, lax.rem(x + d % N_TP, N_TP))

    barrier = pltpu.get_barrier_semaphore()
    for slot in PEERS:
        pl.semaphore_signal(barrier, inc=1, device_id=ep_peer(slot), device_id_type=MESH_ID)
    for d in range(1, N_TP):
        pl.semaphore_signal(barrier, inc=1, device_id=x_peer(d), device_id_type=MESH_ID)

    loads = [
        pltpu.make_async_copy(s, t, load_sem.at[i])
        for i, (s, t) in enumerate(
            [(tok_hbm, normed), (ow_hbm, ow), (sg_hbm, sg), (su_hbm, su), (sd_hbm, sd),
             (wg_hbm, wg), (wu_hbm, wu), (wd_hbm, wd)]
        )
    ]
    for cp in loads:
        cp.start()

    ids = ids_ref[...]
    expert = lax.broadcasted_iota(jnp.int32, (EXPERTS, ROWS), 0)
    first = (expert == ids[0:1, :]).astype(F32)
    second = (expert == ids[1:2, :]).astype(F32)
    s_row = lax.broadcasted_iota(jnp.int32, (ROWS, ROWS), 0)
    s_col = lax.broadcasted_iota(jnp.int32, (ROWS, ROWS), 1)
    earlier = ((s_row < s_col) & ((s_row >> 7) == (s_col >> 7))).astype(F32).astype(BF)
    seen = dot((first + second).astype(BF), earlier)
    rank_a = jnp.sum(first * seen, axis=0, keepdims=True)
    rank_b = jnp.sum(second * seen, axis=0, keepdims=True)
    owner = ids >> 2
    away = ((owner ^ c) & 1) * NZ * NY + (((owner >> 3) - z) & 3) * NY + (((owner >> 1) - y) & 3)
    place = (ids & 3) * SLOTS + away * 16
    place = place + (lax.broadcasted_iota(jnp.int32, (2, ROWS), 1) >> 7) * CAP
    slots[0:1, :] = place[0:1, :].astype(F32) + rank_a
    slots[1:2, :] = place[1:2, :].astype(F32) + rank_b

    with jax.named_scope('wait_tokens'):
        loads[0].wait()

    def norm_step(i, carry):
        rows = pl.ds(pl.multiple_of(i * 64, 64), 64)
        wide = normed[rows, :].astype(F32)
        scale = lax.rsqrt(jnp.mean(wide * wide, axis=-1, keepdims=True) + EPS)
        normed[rows, :] = ((wide * scale) * gain_ref[...]).astype(BF)
        return carry

    with jax.named_scope('norm'):
        lax.fori_loop(0, ROWS // 64, norm_step, 0)

    def slot_rows(base, rows):
        index = lax.broadcasted_iota(jnp.int32, (rows, ROWS), 0) + base
        return index.astype(F32)

    def send_half(buf, to, half, j, send_sem, recv_sem, sign):
        for slot in HALVES[half]:
            rows = pl.ds(slot * 16, 16)
            pltpu.make_async_remote_copy(
                src_ref=buf.at[j, rows], dst_ref=to.at[j, rows],
                send_sem=send_sem.at[2 * j + half], recv_sem=recv_sem.at[2 * j + half],
                device_id=ep_peer(slot, sign), device_id_type=MESH_ID,
            ).start()

    def wait_half(buf, to, h, send_sem, recv_sem):
        for half in range(2):
            @pl.when(lax.rem(h, 2) == half)
            def _():
                rows = pl.ds(0, len(HALVES[half]) * 16)
                pltpu.make_async_remote_copy(
                    src_ref=buf.at[h // 2, rows], dst_ref=to.at[h // 2, rows],
                    send_sem=send_sem.at[h], recv_sem=recv_sem.at[h],
                    device_id=ep_peer(1), device_id_type=MESH_ID,
                ).wait()

    nxt = lax.rem(me + 1, N_EP)
    nxt_dev = (nxt // (NY * NC), lax.rem(nxt // NC, NY), lax.rem(nxt, NC), x)
    halos = [
        pltpu.make_async_remote_copy(
            src_ref=ref.at[pl.ds(ROWS - BLOCK, BLOCK)], dst_ref=halo.at[i],
            send_sem=hsend.at[i], recv_sem=hrecv.at[i],
            device_id=nxt_dev, device_id_type=MESH_ID,
        )
        for i, ref in enumerate((k_ref, v_ref))
    ]

    def gather_step(j, carry):
        index = slot_rows(j * SLOTS, SLOTS)
        pick = (index == slots[0:1, :]) | (index == slots[1:2, :])
        pick = pick.astype(F32).astype(BF)
        for n in range(N_TP):
            cols = slice(n * COLS, (n + 1) * COLS)
            disp_send[j, :, cols] = dot(pick, normed[:, cols]).astype(BF)

        @pl.when(j == 0)
        def _():
            with jax.named_scope('barrier'):
                pl.semaphore_wait(barrier, len(PEERS) + N_TP - 1)
            for cp in halos:
                cp.start()

        with jax.named_scope('send'):
            for half in range(2):
                send_half(disp_send, disp_recv, half, j, dsend, drecv, 1)
        disp_recv[j, 0:16, :] = disp_send[j, 0:16, :]
        return carry

    with jax.named_scope('gather'):
        lax.fori_loop(0, LOCAL, gather_step, 0)

    def x_copy(t, n, src, dst, d):
        return pltpu.make_async_remote_copy(
            src_ref=src, dst_ref=dst, send_sem=xsend.at[t, n], recv_sem=xrecv.at[t, n],
            device_id=x_peer(d), device_id_type=MESH_ID,
        )

    def x_copies(which, t, part, relay, sides):
        routes = (
            (part(2, 0), relay(0), 1),
            (part(2, 1), relay(1), -1),
            (part(1, 1), sides(0, 1), 1),
            (part(-1, 0), sides(1, 0), -1),
            (part(1, 0), sides(0, 0), 1),
            (part(-1, 1), sides(1, 1), -1),
        )
        return [x_copy(t, n, *routes[n]) for n in which]

    def start_first(*refs):
        for cp in x_copies((0, 1, 2, 3), *refs):
            cp.start()

    def start_second(t, part, relay, sides):
        for cp in x_copies((0, 1), t, part, relay, sides):
            cp.wait()
        for n, d in ((0, 1), (1, -1)):
            own = part(d, n)
            own[...] = (own[...].astype(F32) + relay(n)[...].astype(F32)).astype(BF)
        for cp in x_copies((4, 5), t, part, relay, sides):
            cp.start()

    def wait_rest(*refs):
        for cp in x_copies((2, 3, 4, 5), *refs):
            cp.wait()

    def summed(t, part, relay, sides, half):
        return (
            part(0, half)[...].astype(F32)
            + sides(0, half)[...].astype(F32) + sides(1, half)[...].astype(F32)
        )

    def col_block(d):
        return pl.ds(pl.multiple_of(lax.rem(x + d % N_TP, N_TP) * COLS, COLS), COLS)

    def shared_refs():
        half = ROWS // 2
        return (
            2 * LOCAL,
            lambda d, n: sh_send.at[pl.ds(n * half, half), col_block(d)],
            lambda n: sh_relay.at[n],
            lambda s, n: sh_side.at[s, pl.ds(n * half, half)],
        )

    def mixer_refs():
        half = BLOCK // 2

        def part(d, n):
            at = lax.rem(x + d % N_TP, N_TP) * BLOCK + n * half
            return mix_send.at[pl.ds(pl.multiple_of(at, half), half)]

        return (
            2 * LOCAL + 1, part, lambda n: mix_relay.at[n],
            lambda s, n: mix_side.at[s, pl.ds(n * half, half)],
        )

    def expert_refs(h):
        half = HALF // 2
        j, base = h // 2, lax.rem(h, 2) * HALF

        def part(d, n):
            at = pl.multiple_of(base + n * half, half)
            return disp_send.at[j, pl.ds(at, half), col_block(d)]

        return (
            h, part, lambda n: rs_relay.at[h, n],
            lambda s, n: rs_side.at[h, s, pl.ds(n * half, half)],
        )

    loads[2].wait()
    loads[3].wait()
    loads[4].wait()
    gate = dot(normed[...], sg[...])
    up = dot(normed[...], su[...])
    hidden = (gate / (1.0 + jnp.exp(-gate)) * up).astype(BF)
    for n in range(N_TP):
        cols = slice(n * COLS, (n + 1) * COLS)
        sh_send[:, cols] = dot(hidden, sd[:, cols]).astype(BF)

    start_first(*shared_refs())

    lane = lax.broadcasted_iota(jnp.int32, (1, 128), 1)
    low = lane < HEAD_DIM
    half_a = lax.broadcasted_iota(jnp.int32, (128, 128), 0) >> 6
    half_b = lax.broadcasted_iota(jnp.int32, (128, 128), 1) >> 6
    same_half = (half_a == half_b).astype(F32).astype(BF)

    q_gain = jnp.concatenate([qg_ref[...], qg_ref[...]], axis=1)
    k_gain = jnp.concatenate([kg_ref[...], kg_ref[...]], axis=1)

    def head_norm(rows_in, gain):
        wide = rows_in.astype(F32)
        square = wide * wide
        top = square.astype(BF)
        rest = (square - top.astype(F32)).astype(BF)
        total = dot(top, same_half) + dot(rest, same_half)
        scale = lax.rsqrt(total * (1.0 / HEAD_DIM) + EPS)
        return ((wide * scale) * gain).astype(BF)

    def both_halves(rows_in, dst, rows):
        wide = rows_in.astype(F32)
        turned = pltpu.roll(wide, HEAD_DIM, 1)
        dst[0, rows, :] = jnp.where(low, wide, turned).astype(BF)
        dst[1, rows, :] = jnp.where(low, turned, wide).astype(BF)

    own_rows = slice(BLOCK, BLOCK + ROWS)
    both_halves(head_norm(k_ref[...], k_gain), kd, own_rows)
    both_halves(v_ref[...], vd, own_rows)
    with jax.named_scope('halo_wait'):
        for cp in halos:
            cp.wait()
    both_halves(head_norm(halo[0], k_gain), kd, slice(0, BLOCK))
    both_halves(halo[1], vd, slice(0, BLOCK))
    query_pos = lax.broadcasted_iota(jnp.int32, (BLOCK, 2 * BLOCK), 0)
    key_pos = lax.broadcasted_iota(jnp.int32, (BLOCK, 2 * BLOCK), 1)

    def attend(n, carry):
        rows = pl.ds(pl.multiple_of(n * BLOCK, BLOCK), BLOCK)
        band = pl.ds(pl.multiple_of(n * BLOCK, BLOCK), 2 * BLOCK)
        floor = jnp.where(me * 4 + n == 0, BLOCK, 0)
        inside = (key_pos <= query_pos + BLOCK) & (key_pos > query_pos) & (key_pos >= floor)
        for kv in range(2):
            parts = []
            for b in range(2):
                cols = slice((kv * 2 + b) * 128, (kv * 2 + b + 1) * 128)
                qn = head_norm(q_ref[rows, cols], q_gain).astype(F32)
                parts.append(jnp.where(low, qn, 0.0).astype(BF))
                parts.append(jnp.where(low, 0.0, qn).astype(BF))
            stacked = jnp.concatenate(parts, axis=0)
            scores = lax.dot_general(
                stacked, kd[kv, band, :], (((1,), (1,)), ((), ())), preferred_element_type=F32
            ) * 0.125
            probs = []
            for g in range(4):
                sink = sink_ref[0, kv * 4 + g]
                part = jnp.where(inside, scores[g * BLOCK:(g + 1) * BLOCK], MASKED)
                top = jnp.maximum(jnp.max(part, axis=-1, keepdims=True), sink)
                ex = jnp.exp(part - top)
                den = jnp.sum(ex, axis=-1, keepdims=True) + jnp.exp(sink - top)
                probs.append((ex * (1.0 / den)).astype(BF))
            mixed = dot(jnp.concatenate(probs, axis=0), vd[kv, band, :])
            for b in range(2):
                lo = mixed[(2 * b) * BLOCK:(2 * b + 1) * BLOCK]
                hi = mixed[(2 * b + 1) * BLOCK:(2 * b + 2) * BLOCK]
                cols = slice((kv * 2 + b) * 128, (kv * 2 + b + 1) * 128)
                heads[rows, cols] = jnp.where(low, lo, hi).astype(BF)
        return carry

    with jax.named_scope('attend'):
        lax.fori_loop(0, ROWS // BLOCK, attend, 0)
    loads[1].wait()
    for n in range(N_TP):
        cols = slice(n * COLS, (n + 1) * COLS)
        mix_send[:, cols] = dot(heads[...], ow[:, cols]).astype(BF)

    start_first(*mixer_refs())
    with jax.named_scope('shared2'):
        start_second(*shared_refs())

    loads[5].wait()
    loads[6].wait()
    loads[7].wait()

    def combine(h, carry):
        with jax.named_scope('wait_ret'):
            wait_half(ret_send, ret_recv, h, tsend, trecv)
        with jax.named_scope('combine'):
            index = slot_rows(h * HALF, HALF)
            weight = jnp.where(index == slots[0:1, :], rw_ref[0:1, :], 0.0)
            weight = weight + jnp.where(index == slots[1:2, :], rw_ref[1:2, :], 0.0)
            main = weight.astype(BF)
            rest = (weight - main.astype(F32)).astype(BF)
            dims = (((0,), (0,)), ((), ()))
            back = ret_recv[h // 2, pl.ds(pl.multiple_of(lax.rem(h, 2) * HALF, HALF), HALF), :]
            acc[...] += lax.dot_general(
                main, back, dims, preferred_element_type=F32
            ) + lax.dot_general(rest, back, dims, preferred_element_type=F32)
        return carry

    def step(i, carry):
        @pl.when(i < 2 * LOCAL)
        def _():
            with jax.named_scope('wait_disp'):
                wait_half(disp_send, disp_recv, i, dsend, drecv)
            j = i // 2
            rows = pl.ds(pl.multiple_of(lax.rem(i, 2) * HALF, HALF), HALF)
            with jax.named_scope('ffn'):
                came = disp_recv[j, rows, :]
                gate = dot(came, wg[j])
                up = dot(came, wu[j])
                hidden = (gate / (1.0 + jnp.exp(-gate)) * up).astype(BF)
                for n in range(N_TP):
                    cols = slice(n * COLS, (n + 1) * COLS)
                    disp_send[j, rows, cols] = dot(hidden, wd[j, :, cols]).astype(BF)
            start_first(*expert_refs(i))

        @pl.when(i == 2)
        def _():
            with jax.named_scope('mix2'):
                start_second(*mixer_refs())

        @pl.when((i >= 1) & (i <= 2 * LOCAL))
        def _():
            with jax.named_scope('rs2'):
                start_second(*expert_refs(i - 1))

        @pl.when(i == 2 * LOCAL)
        def _():
            with jax.named_scope('mix_out'):
                wait_rest(*mixer_refs())
                for half in range(2):
                    rows = slice(half * BLOCK // 2, (half + 1) * BLOCK // 2)
                    mix_out[rows, :] = summed(*mixer_refs(), half).astype(BF)

        @pl.when((i >= 2) & (i <= 2 * LOCAL + 1))
        def _():
            h = i - 2
            j, base = h // 2, lax.rem(h, 2) * HALF
            with jax.named_scope('wait_rs'):
                wait_rest(*expert_refs(h))
            with jax.named_scope('ret'):
                for half in range(2):
                    at = pl.multiple_of(base + half * HALF // 2, HALF // 2)
                    ret_send[j, pl.ds(at, HALF // 2), :] = summed(
                        *expert_refs(h), half
                    ).astype(BF)
                for half in range(2):
                    @pl.when(lax.rem(h, 2) == half)
                    def _():
                        send_half(ret_send, ret_recv, half, j, tsend, trecv, -1)

            @pl.when(lax.rem(h, 2) == 0)
            def _():
                ret_recv[j, 0:16, :] = ret_send[j, 0:16, :]

        @pl.when(i == 3)
        def _():
            with jax.named_scope('wait_shared'):
                wait_rest(*shared_refs())
            for half in range(2):
                rows = slice(half * ROWS // 2, (half + 1) * ROWS // 2)
                acc[rows, :] = summed(*shared_refs(), half).astype(BF).astype(F32)

        low_h = jnp.where(i < 2 * LOCAL, 0, jnp.where(i == 2 * LOCAL, 0, jnp.where(i == 2 * LOCAL + 1, 3, 7)))
        high_h = jnp.where(i < 2 * LOCAL, 0, jnp.where(i == 2 * LOCAL, 3, jnp.where(i == 2 * LOCAL + 1, 7, 8)))
        lax.fori_loop(low_h, high_h, combine, 0)
        return carry

    lax.fori_loop(0, 2 * LOCAL + 3, step, 0)

    def quarter(d):
        at = lax.rem(x + d % N_TP, N_TP) * BLOCK
        return pl.ds(pl.multiple_of(at, BLOCK), BLOCK)

    fin_send[...] = acc[...].astype(BF)
    finals = [
        pltpu.make_async_remote_copy(
            src_ref=fin_send.at[quarter(d)], dst_ref=fin_recv.at[d - 1],
            send_sem=fsend.at[d - 1], recv_sem=frecv.at[d - 1],
            device_id=x_peer(d), device_id_type=MESH_ID,
        )
        for d in range(1, N_TP)
    ]
    for cp in finals:
        cp.start()
    exp_out[:, col_block(0)] = fin_send[quarter(0), :]
    for d in (1, 3, 2):
        with jax.named_scope('wait_fin'):
            finals[d - 1].wait()
        exp_out[:, col_block(-d)] = fin_recv[d - 1]


def shards(
    query_rows, key_rows, value_rows, query_gain, key_gain, sink_logit, out_weight, tokens,
    norm_gain, expert_ids, route_weight, gate_weight, up_weight, down_weight,
    shared_gate, shared_up, shared_down,
):
    vmem = pl.BlockSpec(memory_space=pltpu.VMEM)
    hbm = pl.BlockSpec(memory_space=pl.ANY)
    smem = pl.BlockSpec(memory_space=pltpu.SMEM)
    dma = pltpu.SemaphoreType.DMA
    out = jax.ShapeDtypeStruct((BLOCK, D), BF)
    return pl.pallas_call(
        layer_kernel,
        out_shape=(out, out),
        in_specs=[vmem] * 5 + [smem] + [vmem] * 3 + [hbm] * 8,
        out_specs=(vmem, vmem),
        scratch_shapes=[
            pltpu.VMEM((ROWS, D), BF),
            pltpu.VMEM((ROWS, D), BF),
            pltpu.VMEM((LOCAL, D, FFS), BF),
            pltpu.VMEM((LOCAL, D, FFS), BF),
            pltpu.VMEM((LOCAL, FFS, D), BF),
            pltpu.VMEM((D, FFS), BF),
            pltpu.VMEM((D, FFS), BF),
            pltpu.VMEM((FFS, D), BF),
            pltpu.VMEM((2, ROWS), F32),
            pltpu.VMEM((LOCAL, SLOTS, D), BF),
            pltpu.VMEM((LOCAL, SLOTS, D), BF),
            pltpu.VMEM((2 * LOCAL, 2, HALF // 2, COLS), BF),
            pltpu.VMEM((2 * LOCAL, 2, HALF, COLS), BF),
            pltpu.VMEM((LOCAL, SLOTS, COLS), BF),
            pltpu.VMEM((LOCAL, SLOTS, COLS), BF),
            pltpu.VMEM((ROWS, D), BF),
            pltpu.VMEM((2, BLOCK // 2, D), BF),
            pltpu.VMEM((2, BLOCK, D), BF),
            pltpu.VMEM((ROWS, D), BF),
            pltpu.VMEM((2, ROWS // 2, COLS), BF),
            pltpu.VMEM((2, ROWS, COLS), BF),
            pltpu.VMEM((ROWS, COLS), F32),
            pltpu.VMEM((ROWS, COLS), BF),
            pltpu.VMEM((N_TP - 1, BLOCK, COLS), BF),
            pltpu.VMEM((2, BLOCK, 128), BF),
            pltpu.VMEM((2, BLOCK + ROWS, 128), BF),
            pltpu.VMEM((2, BLOCK + ROWS, 128), BF),
            pltpu.VMEM((ROWS, 512), BF),
            dma((8,)),
            dma((2 * LOCAL,)), dma((2 * LOCAL,)),
            dma((2 * LOCAL + 2, 6)), dma((2 * LOCAL + 2, 6)),
            dma((2 * LOCAL,)), dma((2 * LOCAL,)),
            dma((N_TP - 1,)), dma((N_TP - 1,)),
            dma((2,)), dma((2,)),
        ],
        compiler_params=pltpu.CompilerParams(
            collective_id=0, has_side_effects=True, vmem_limit_bytes=67000000
        ),
        name="layer",
    )(
        query_rows, key_rows, value_rows,
        query_gain[None], key_gain[None],
        sink_logit[None], norm_gain[None], expert_ids.T, route_weight.T,
        tokens, out_weight, gate_weight, up_weight, down_weight,
        shared_gate, shared_up, shared_down,
    )


def solution(mesh):
    split = Mesh(mesh.devices.reshape(NZ, NY, NC, mesh.shape["tp"]), EP_TP)
    return jax.shard_map(
        shards,
        mesh=split,
        in_specs=(
            P(EP, "x"), P(EP, "x"), P(EP, "x"), P(), P(), P("x"), P("x", None),
            P(EP, None), P(), P(EP, None), P(EP, None),
            P(EP, None, "x"), P(EP, None, "x"), P(EP, "x", None),
            P(None, "x"), P(None, "x"), P("x", None),
        ),
        out_specs=(P(EP_TP, None), P(EP_TP, None)),
        check_vma=False,
    )
```

```python
import jax
import jax.numpy as jnp
from jax import lax
from jax.experimental import pallas as pl
from jax.experimental.pallas import tpu as pltpu
from jax.sharding import Mesh
from jax.sharding import PartitionSpec as P

HEADS = 32
KV_HEADS = 8
HEAD_DIM = 64
BLOCK = 128
CAP = 4
N_TP = 4
NZ, NY, NC = 4, 4, 2
N_EP = NZ * NY * NC
EP = ("z", "y", "c")
EP_TP = ("z", "y", "c", "x")
D = 2048
ROWS = 512
FFS = 256
EXPERTS = 128
LOCAL = 4
COLS = D // N_TP
EPS = 1e-06
MASKED = -1e30
MESH_ID = pl.DeviceIdType.MESH
BF = jnp.bfloat16
F32 = jnp.float32

CHUNKS = N_EP // 4
CHUNK = 4 * LOCAL * 16
QUARTER = CHUNK // N_TP


def dot(a, b):
    return jnp.dot(a, b, preferred_element_type=F32)


def layer_kernel(
    q_ref, k_ref, v_ref, qg_ref, kg_ref, sink_ref, gain_ref, ids_ref, rw_ref,
    tok_hbm, ow_hbm, wg_hbm, wu_hbm, wd_hbm, sg_hbm, su_hbm, sd_hbm,
    mix_out, exp_out,
    normed, ow, wg, wu, wd, sg, su, sd,
    slots, disp_send, disp_recv, rs_relay, rs_side, ret_send, ret_recv,
    mix_send, mix_relay, mix_side, sh_send, sh_relay, sh_side, acc, turn,
    halo, kd, vd, heads,
    load_sem, dsend, drecv, xsend, xrecv, tsend, trecv, hsend, hrecv,
):
    z, y, c, x = (lax.axis_index(a) for a in EP_TP)
    me = (z * NY + y) * NC + c

    def ep_peer(chunk, k, sign=1):
        dc, dz = chunk // 4, lax.rem(chunk + k, 4)
        if sign < 0:
            dz = NZ - dz
        return (lax.rem(z + dz, NZ), lax.rem(y + (k * sign) % NY, NY), lax.rem(c + dc, NC), x)

    def x_peer(d):
        return (z, y, c, lax.rem(x + d % N_TP, N_TP))

    barrier = pltpu.get_barrier_semaphore()
    for owner in range(1, N_EP):
        pl.semaphore_signal(
            barrier, inc=1, device_id=ep_peer(owner // 4, owner % 4), device_id_type=MESH_ID
        )
    for d in range(1, N_TP):
        pl.semaphore_signal(barrier, inc=1, device_id=x_peer(d), device_id_type=MESH_ID)

    loads = [
        pltpu.make_async_copy(s, t, load_sem.at[i])
        for i, (s, t) in enumerate(
            [(tok_hbm, normed), (sg_hbm, sg), (su_hbm, su), (sd_hbm, sd), (ow_hbm, ow),
             (wg_hbm, wg), (wu_hbm, wu), (wd_hbm, wd)]
        )
    ]
    loads[0].start()

    ids = ids_ref[...]
    expert = lax.broadcasted_iota(jnp.int32, (EXPERTS, ROWS), 0)
    first = (expert == ids[0:1, :]).astype(F32)
    second = (expert == ids[1:2, :]).astype(F32)
    s_row = lax.broadcasted_iota(jnp.int32, (ROWS, ROWS), 0)
    s_col = lax.broadcasted_iota(jnp.int32, (ROWS, ROWS), 1)
    earlier = ((s_row < s_col) & ((s_row >> 7) == (s_col >> 7))).astype(F32).astype(BF)
    seen = dot((first + second).astype(BF), earlier)
    rank_a = jnp.sum(first * seen, axis=0, keepdims=True)
    rank_b = jnp.sum(second * seen, axis=0, keepdims=True)
    owner = ids >> 2
    dy = ((owner >> 1) - y) & 3
    chunk_at = ((owner ^ c) & 1) * 4 + (((owner >> 3) - z - dy) & 3)
    block_at = lax.broadcasted_iota(jnp.int32, (2, ROWS), 1) >> 7
    rank = jnp.concatenate([rank_a, rank_b], axis=0)
    sent_at = chunk_at * CHUNK + (ids & 3) * 64 + dy * 16 + block_at * CAP
    back_at = chunk_at * QUARTER + dy * 16 + (ids & 3) * CAP
    slots[0:2, :] = sent_at.astype(F32) + rank
    slots[2:4, :] = back_at.astype(F32) + rank

    p_row = lax.broadcasted_iota(jnp.int32, (CHUNK, CHUNK), 0)
    p_col = lax.broadcasted_iota(jnp.int32, (CHUNK, CHUNK), 1)
    p_from = ((p_row >> 2) & 3) * 64 + ((p_row >> 4) & 3) * 16 + (p_row >> 6) * 4 + (p_row & 3)
    turn[...] = (p_from == p_col).astype(F32).astype(BF)

    with jax.named_scope('wait_tokens'):
        loads[0].wait()
    for cp in loads[1:]:
        cp.start()

    def norm_step(i, carry):
        rows = pl.ds(pl.multiple_of(i * 64, 64), 64)
        wide = normed[rows, :].astype(F32)
        scale = lax.rsqrt(jnp.mean(wide * wide, axis=-1, keepdims=True) + EPS)
        normed[rows, :] = ((wide * scale) * gain_ref[...]).astype(BF)
        return carry

    with jax.named_scope('norm'):
        lax.fori_loop(0, ROWS // 64, norm_step, 0)

    def slot_rows(base, shape):
        return (lax.broadcasted_iota(jnp.int32, shape, 0) + base).astype(F32)

    def send_chunk(i):
        for j in range(LOCAL):
            for k in range(4):
                rows = pl.ds(j * 64 + k * 16, 16)

                def start(rows=rows, k=k):
                    pltpu.make_async_remote_copy(
                        src_ref=disp_send.at[i, rows], dst_ref=disp_recv.at[i, rows],
                        send_sem=dsend.at[i], recv_sem=drecv.at[i],
                        device_id=ep_peer(i, k), device_id_type=MESH_ID,
                    ).start()

                if k:
                    start()
                else:
                    pl.when(i > 0)(start)

    def send_back(i):
        for k in range(4):
            rows = pl.ds(k * 16, 16)

            def start(rows=rows, k=k):
                pltpu.make_async_remote_copy(
                    src_ref=ret_send.at[i, rows], dst_ref=ret_recv.at[i, rows],
                    send_sem=tsend.at[i], recv_sem=trecv.at[i],
                    device_id=ep_peer(i, k, -1), device_id_type=MESH_ID,
                ).start()

            if k:
                start()
            else:
                pl.when(i > 0)(start)

    def wait_chunk(buf, to, i, send_sem, recv_sem):
        rows_in = buf.shape[1]

        def wait(count):
            rows = pl.ds(0, count)
            pltpu.make_async_remote_copy(
                src_ref=buf.at[i, rows], dst_ref=to.at[i, rows],
                send_sem=send_sem.at[i], recv_sem=recv_sem.at[i],
                device_id=ep_peer(0, 1), device_id_type=MESH_ID,
            ).wait()

        pl.when(i == 0)(lambda: wait(rows_in * 3 // 4))
        pl.when(i > 0)(lambda: wait(rows_in))

    nxt = lax.rem(me + 1, N_EP)
    nxt_dev = (nxt // (NY * NC), lax.rem(nxt // NC, NY), lax.rem(nxt, NC), x)
    halos = [
        pltpu.make_async_remote_copy(
            src_ref=ref.at[pl.ds(ROWS - BLOCK, BLOCK)], dst_ref=halo.at[i],
            send_sem=hsend.at[i], recv_sem=hrecv.at[i],
            device_id=nxt_dev, device_id_type=MESH_ID,
        )
        for i, ref in enumerate((k_ref, v_ref))
    ]

    def gather_step(i, carry):
        index = slot_rows(i * CHUNK, (CHUNK, ROWS))
        pick = (index == slots[0:1, :]) | (index == slots[1:2, :])
        pick = pick.astype(F32).astype(BF)
        for n in range(N_TP):
            cols = slice(n * COLS, (n + 1) * COLS)
            disp_send[i, :, cols] = dot(pick, normed[:, cols]).astype(BF)

        if carry is None:
            with jax.named_scope('barrier'):
                pl.semaphore_wait(barrier, N_EP - 1 + N_TP - 1)
            for cp in halos:
                cp.start()
        with jax.named_scope('send'):
            send_chunk(i)
        return carry

    gather_step(0, None)
    for j in range(LOCAL):
        rows = slice(j * 64, j * 64 + 16)
        disp_recv[0, rows, :] = disp_send[0, rows, :]


    def x_copy(t, n, src, dst, d):
        return pltpu.make_async_remote_copy(
            src_ref=src, dst_ref=dst, send_sem=xsend.at[t, n], recv_sem=xrecv.at[t, n],
            device_id=x_peer(d), device_id_type=MESH_ID,
        )

    def x_copies(which, t, part, relay, sides):
        routes = (
            (part(2, 0), relay(0), 1),
            (part(2, 1), relay(1), -1),
            (part(1, 1), sides(0, 1), 1),
            (part(-1, 0), sides(1, 0), -1),
            (part(1, 0), sides(0, 0), 1),
            (part(-1, 1), sides(1, 1), -1),
        )
        return [x_copy(t, n, *routes[n]) for n in which]

    def start_first(*refs):
        for cp in x_copies((0, 1, 2, 3), *refs):
            cp.start()

    def start_second(t, part, relay, sides):
        for cp in x_copies((0, 1), t, part, relay, sides):
            cp.wait()
        for n, d in ((0, 1), (1, -1)):
            own = part(d, n)
            own[...] = (own[...].astype(F32) + relay(n)[...].astype(F32)).astype(BF)
        for cp in x_copies((4, 5), t, part, relay, sides):
            cp.start()

    def wait_rest(*refs):
        for cp in x_copies((2, 3, 4, 5), *refs):
            cp.wait()

    def summed(t, part, relay, sides, half):
        return (
            part(0, half)[...].astype(F32)
            + sides(0, half)[...].astype(F32) + sides(1, half)[...].astype(F32)
        )

    def by_quarter(t, buf, rows_in, relay, side):
        half = rows_in // 2

        def part(d, n):
            at = lax.rem(x + d % N_TP, N_TP) * rows_in + n * half
            return buf.at[pl.ds(pl.multiple_of(at, half), half)]

        return (
            t, part, lambda n: relay.at[n],
            lambda s, n: side.at[s, pl.ds(n * half, half)],
        )

    def shared_refs():
        return by_quarter(CHUNKS, sh_send, BLOCK, sh_relay, sh_side)

    def mixer_refs():
        return by_quarter(CHUNKS + 1, mix_send, BLOCK, mix_relay, mix_side)

    def expert_refs(i):
        return by_quarter(i, disp_send.at[i], QUARTER, rs_relay.at[i], rs_side.at[i])

    for cp in loads[1:4]:
        cp.wait()
    gate = dot(normed[...], sg[...])
    up = dot(normed[...], su[...])
    hidden = (gate / (1.0 + jnp.exp(-gate)) * up).astype(BF)
    for n in range(N_TP):
        cols = slice(n * COLS, (n + 1) * COLS)
        sh_send[:, cols] = dot(hidden, sd[:, cols]).astype(BF)

    start_first(*shared_refs())
    with jax.named_scope('gather'):
        lax.fori_loop(1, CHUNKS, gather_step, 0)

    lane = lax.broadcasted_iota(jnp.int32, (1, 128), 1)
    low = lane < HEAD_DIM
    half_a = lax.broadcasted_iota(jnp.int32, (128, 128), 0) >> 6
    half_b = lax.broadcasted_iota(jnp.int32, (128, 128), 1) >> 6
    same_half = (half_a == half_b).astype(F32).astype(BF)

    q_gain = jnp.concatenate([qg_ref[...], qg_ref[...]], axis=1)
    k_gain = jnp.concatenate([kg_ref[...], kg_ref[...]], axis=1)

    def head_norm(rows_in, gain):
        wide = rows_in.astype(F32)
        square = wide * wide
        top = square.astype(BF)
        rest = (square - top.astype(F32)).astype(BF)
        total = dot(top, same_half) + dot(rest, same_half)
        scale = lax.rsqrt(total * (1.0 / HEAD_DIM) + EPS)
        return ((wide * scale) * gain).astype(BF)

    def both_halves(rows_in, dst, rows):
        wide = rows_in.astype(F32)
        turned = pltpu.roll(wide, HEAD_DIM, 1)
        dst[0, rows, :] = jnp.where(low, wide, turned).astype(BF)
        dst[1, rows, :] = jnp.where(low, turned, wide).astype(BF)

    own_rows = slice(BLOCK, BLOCK + ROWS)
    both_halves(head_norm(k_ref[...], k_gain), kd, own_rows)
    both_halves(v_ref[...], vd, own_rows)
    with jax.named_scope('halo_wait'):
        for cp in halos:
            cp.wait()
    both_halves(head_norm(halo[0], k_gain), kd, slice(0, BLOCK))
    both_halves(halo[1], vd, slice(0, BLOCK))
    query_pos = lax.broadcasted_iota(jnp.int32, (BLOCK, 2 * BLOCK), 0)
    key_pos = lax.broadcasted_iota(jnp.int32, (BLOCK, 2 * BLOCK), 1)

    def attend(n, carry):
        rows = pl.ds(pl.multiple_of(n * BLOCK, BLOCK), BLOCK)
        band = pl.ds(pl.multiple_of(n * BLOCK, BLOCK), 2 * BLOCK)
        floor = jnp.where(me * 4 + n == 0, BLOCK, 0)
        inside = (key_pos <= query_pos + BLOCK) & (key_pos > query_pos) & (key_pos >= floor)
        for kv in range(2):
            parts = []
            for b in range(2):
                cols = slice((kv * 2 + b) * 128, (kv * 2 + b + 1) * 128)
                qn = head_norm(q_ref[rows, cols], q_gain).astype(F32)
                parts.append(jnp.where(low, qn, 0.0).astype(BF))
                parts.append(jnp.where(low, 0.0, qn).astype(BF))
            stacked = jnp.concatenate(parts, axis=0)
            scores = lax.dot_general(
                stacked, kd[kv, band, :], (((1,), (1,)), ((), ())), preferred_element_type=F32
            ) * 0.125
            probs = []
            for g in range(4):
                sink = sink_ref[0, kv * 4 + g]
                part = jnp.where(inside, scores[g * BLOCK:(g + 1) * BLOCK], MASKED)
                top = jnp.maximum(jnp.max(part, axis=-1, keepdims=True), sink)
                ex = jnp.exp(part - top)
                den = jnp.sum(ex, axis=-1, keepdims=True) + jnp.exp(sink - top)
                probs.append((ex * (1.0 / den)).astype(BF))
            mixed = dot(jnp.concatenate(probs, axis=0), vd[kv, band, :])
            for b in range(2):
                lo = mixed[(2 * b) * BLOCK:(2 * b + 1) * BLOCK]
                hi = mixed[(2 * b + 1) * BLOCK:(2 * b + 2) * BLOCK]
                cols = slice((kv * 2 + b) * 128, (kv * 2 + b + 1) * 128)
                heads[rows, cols] = jnp.where(low, lo, hi).astype(BF)
        return carry

    with jax.named_scope('attend'):
        lax.fori_loop(0, ROWS // BLOCK, attend, 0)
    loads[4].wait()
    for n in range(N_TP):
        cols = slice(n * COLS, (n + 1) * COLS)
        mix_send[:, cols] = dot(heads[...], ow[:, cols]).astype(BF)

    start_first(*mixer_refs())
    with jax.named_scope('shared2'):
        start_second(*shared_refs())

    loads[5].wait()
    loads[6].wait()
    loads[7].wait()

    own_tokens = pl.ds(pl.multiple_of(x * BLOCK, BLOCK), BLOCK)

    def combine(i, carry):
        with jax.named_scope('wait_ret'):
            wait_chunk(ret_send, ret_recv, i, tsend, trecv)
        with jax.named_scope('combine'):
            index = slot_rows(i * QUARTER, (QUARTER, BLOCK))
            weight = jnp.where(index == slots[2:3, own_tokens], rw_ref[0:1, own_tokens], 0.0)
            weight += jnp.where(index == slots[3:4, own_tokens], rw_ref[1:2, own_tokens], 0.0)
            main = weight.astype(BF)
            rest = (weight - main.astype(F32)).astype(BF)
            dims = (((0,), (0,)), ((), ()))
            acc[...] += lax.dot_general(
                main, ret_recv[i], dims, preferred_element_type=F32
            ) + lax.dot_general(rest, ret_recv[i], dims, preferred_element_type=F32)
        return carry

    def step(i, carry):
        @pl.when(i < CHUNKS)
        def _():
            with jax.named_scope('wait_disp'):
                wait_chunk(disp_send, disp_recv, i, dsend, drecv)
            with jax.named_scope('ffn'):
                wide = []
                for j in range(LOCAL):
                    came = disp_recv[i, j * 64:(j + 1) * 64, :]
                    gate = dot(came, wg[j])
                    up = dot(came, wu[j])
                    hidden = (gate / (1.0 + jnp.exp(-gate)) * up).astype(BF)
                    wide.append(dot(turn[:, j * 64:(j + 1) * 64], hidden).astype(BF))
                wide = jnp.concatenate(wide, axis=1)
                for n in range(N_TP):
                    cols = slice(n * COLS, (n + 1) * COLS)
                    disp_send[i, :, cols] = dot(wide, wd[:, cols]).astype(BF)
            start_first(*expert_refs(i))

        @pl.when(i == 2)
        def _():
            with jax.named_scope('mix2'):
                start_second(*mixer_refs())

        @pl.when((i >= 1) & (i <= CHUNKS))
        def _():
            with jax.named_scope('rs2'):
                start_second(*expert_refs(i - 1))

        @pl.when(i == CHUNKS)
        def _():
            with jax.named_scope('mix_out'):
                wait_rest(*mixer_refs())
                for half in range(2):
                    rows = slice(half * BLOCK // 2, (half + 1) * BLOCK // 2)
                    mix_out[rows, :] = summed(*mixer_refs(), half).astype(BF)

        @pl.when((i >= 2) & (i <= CHUNKS + 1))
        def _():
            h = i - 2
            with jax.named_scope('wait_rs'):
                wait_rest(*expert_refs(h))
            with jax.named_scope('ret'):
                for half in range(2):
                    rows = slice(half * QUARTER // 2, (half + 1) * QUARTER // 2)
                    ret_send[h, rows, :] = summed(*expert_refs(h), half).astype(BF)
                send_back(h)

            @pl.when(h == 0)
            def _():
                ret_recv[0, 0:16, :] = ret_send[0, 0:16, :]

        @pl.when(i == 3)
        def _():
            with jax.named_scope('wait_shared'):
                wait_rest(*shared_refs())
            for half in range(2):
                rows = slice(half * BLOCK // 2, (half + 1) * BLOCK // 2)
                acc[rows, :] = summed(*shared_refs(), half).astype(BF).astype(F32)

        first_h = jnp.where(i <= CHUNKS, 0, jnp.where(i == CHUNKS + 1, 3, 7))
        last_h = jnp.where(i < CHUNKS, 0, jnp.where(i == CHUNKS, 3, jnp.where(i == CHUNKS + 1, 7, 8)))
        lax.fori_loop(first_h, last_h, combine, 0)
        return carry

    lax.fori_loop(0, CHUNKS + 3, step, 0)
    exp_out[...] = acc[...].astype(BF)


def hand_over(mix_in, exp_in, mix_out, exp_out):
    mix_out[...] = mix_in[...]
    exp_out[...] = exp_in[...]


def shards(
    query_rows, key_rows, value_rows, query_gain, key_gain, sink_logit, out_weight, tokens,
    norm_gain, expert_ids, route_weight, gate_weight, up_weight, down_weight,
    shared_gate, shared_up, shared_down,
):
    vmem = pl.BlockSpec(memory_space=pltpu.VMEM)
    hbm = pl.BlockSpec(memory_space=pl.ANY)
    smem = pl.BlockSpec(memory_space=pltpu.SMEM)
    dma = pltpu.SemaphoreType.DMA
    out = jax.ShapeDtypeStruct((BLOCK, D), BF)
    results = pl.pallas_call(
        layer_kernel,
        out_shape=(out, out),
        in_specs=[vmem] * 5 + [smem] + [vmem] * 3 + [hbm] * 8,
        out_specs=(vmem, vmem),
        scratch_shapes=[
            pltpu.VMEM((ROWS, D), BF),
            pltpu.VMEM((ROWS, D), BF),
            pltpu.VMEM((LOCAL, D, FFS), BF),
            pltpu.VMEM((LOCAL, D, FFS), BF),
            pltpu.VMEM((LOCAL * FFS, D), BF),
            pltpu.VMEM((D, FFS), BF),
            pltpu.VMEM((D, FFS), BF),
            pltpu.VMEM((FFS, D), BF),
            pltpu.VMEM((4, ROWS), F32),
            pltpu.VMEM((CHUNKS, CHUNK, D), BF),
            pltpu.VMEM((CHUNKS, CHUNK, D), BF),
            pltpu.VMEM((CHUNKS, 2, QUARTER // 2, D), BF),
            pltpu.VMEM((CHUNKS, 2, QUARTER, D), BF),
            pltpu.VMEM((CHUNKS, QUARTER, D), BF),
            pltpu.VMEM((CHUNKS, QUARTER, D), BF),
            pltpu.VMEM((ROWS, D), BF),
            pltpu.VMEM((2, BLOCK // 2, D), BF),
            pltpu.VMEM((2, BLOCK, D), BF),
            pltpu.VMEM((ROWS, D), BF),
            pltpu.VMEM((2, BLOCK // 2, D), BF),
            pltpu.VMEM((2, BLOCK, D), BF),
            pltpu.VMEM((BLOCK, D), F32),
            pltpu.VMEM((CHUNK, CHUNK), BF),
            pltpu.VMEM((2, BLOCK, 128), BF),
            pltpu.VMEM((2, BLOCK + ROWS, 128), BF),
            pltpu.VMEM((2, BLOCK + ROWS, 128), BF),
            pltpu.VMEM((ROWS, 512), BF),
            dma((8,)),
            dma((CHUNKS,)), dma((CHUNKS,)),
            dma((CHUNKS + 2, 6)), dma((CHUNKS + 2, 6)),
            dma((CHUNKS,)), dma((CHUNKS,)),
            dma((2,)), dma((2,)),
        ],
        compiler_params=pltpu.CompilerParams(
            collective_id=0, has_side_effects=True, vmem_limit_bytes=67000000
        ),
        name="layer",
    )(
        query_rows, key_rows, value_rows,
        query_gain[None], key_gain[None],
        sink_logit[None], norm_gain[None], expert_ids.T, route_weight.T,
        tokens, out_weight, gate_weight, up_weight, down_weight.reshape(LOCAL * FFS, D),
        shared_gate, shared_up, shared_down,
    )
    return tuple(
        pl.pallas_call(
            hand_over, out_shape=(out, out), in_specs=[vmem] * 2, out_specs=(vmem, vmem),
            name="hand_over",
        )(*results)
    )


def solution(mesh):
    split = Mesh(mesh.devices.reshape(NZ, NY, NC, mesh.shape["tp"]), EP_TP)
    return jax.shard_map(
        shards,
        mesh=split,
        in_specs=(
            P(EP, "x"), P(EP, "x"), P(EP, "x"), P(), P(), P("x"), P("x", None),
            P(EP, None), P(), P(EP, None), P(EP, None),
            P(EP, None, "x"), P(EP, None, "x"), P(EP, "x", None),
            P(None, "x"), P(None, "x"), P("x", None),
        ),
        out_specs=(P(EP_TP, None), P(EP_TP, None)),
        check_vma=False,
    )
```

```python
import jax
import jax.numpy as jnp
from jax import lax
from jax.experimental import pallas as pl
from jax.experimental.pallas import tpu as pltpu
from jax.sharding import Mesh
from jax.sharding import PartitionSpec as P

HEADS = 32
KV_HEADS = 8
HEAD_DIM = 64
BLOCK = 128
CAP = 4
N_TP = 4
NZ, NY, NC = 4, 4, 2
N_EP = NZ * NY * NC
EP = ("z", "y", "c")
EP_TP = ("z", "y", "c", "x")
D = 2048
ROWS = 512
FFS = 256
EXPERTS = 128
LOCAL = 4
COLS = D // N_TP
EPS = 1e-06
MASKED = -1e30
MESH_ID = pl.DeviceIdType.MESH
BF = jnp.bfloat16
F32 = jnp.float32

CHUNKS = N_EP // 4
CHUNK = 4 * LOCAL * 16
QUARTER = CHUNK // N_TP


def dot(a, b):
    return jnp.dot(a, b, preferred_element_type=F32)


def layer_kernel(
    q_ref, k_ref, v_ref, qg_ref, kg_ref, sink_ref, gain_ref, ids_ref, rw_ref,
    tok_hbm, ow_hbm, wg_hbm, wu_hbm, wd_hbm, sg_hbm, su_hbm, sd_hbm,
    mix_out, exp_out,
    normed, ow, wg, wu, wd, sg, su, sd,
    slots, disp_send, disp_recv, rs_relay, rs_side, ret_send, ret_recv,
    mix_send, mix_relay, mix_side, sh_send, sh_relay, sh_side, acc, turn,
    halo, kd, vd, heads,
    load_sem, dsend, drecv, gsend, grecv, xsend, xrecv, tsend, trecv, hsend, hrecv,
):
    z, y, c, x = (lax.axis_index(a) for a in EP_TP)
    me = (z * NY + y) * NC + c

    def ep_peer(chunk, k, sign=1):
        g, dc = lax.rem(chunk, 4), chunk // 4
        latin = (g + 3) // 4
        both = 2 * (k // 2) + dc
        dy = latin * k + (1 - latin) * both
        dz = latin * lax.rem(g + k, 4) + (1 - latin) * both
        dc = latin * dc + (1 - latin) * (k % 2)
        if sign < 0:
            dy, dz = NY - dy, NZ - dz
        return (lax.rem(z + dz, NZ), lax.rem(y + dy, NY), lax.rem(c + dc, NC), x)

    def x_peer(d):
        return (z, y, c, lax.rem(x + d % N_TP, N_TP))

    barrier = pltpu.get_barrier_semaphore()
    for owner in range(1, N_EP):
        pl.semaphore_signal(
            barrier, inc=1, device_id=ep_peer(owner // 4, owner % 4), device_id_type=MESH_ID
        )
    for d in range(1, N_TP):
        pl.semaphore_signal(barrier, inc=1, device_id=x_peer(d), device_id_type=MESH_ID)

    loads = [
        pltpu.make_async_copy(s, t, load_sem.at[i])
        for i, (s, t) in enumerate(
            [(tok_hbm, normed), (sg_hbm, sg), (su_hbm, su), (sd_hbm, sd), (ow_hbm, ow),
             (wg_hbm, wg), (wu_hbm, wu), (wd_hbm, wd)]
        )
    ]
    loads[0].start()

    ids = ids_ref[...]
    expert = lax.broadcasted_iota(jnp.int32, (EXPERTS, ROWS), 0)
    first = (expert == ids[0:1, :]).astype(F32)
    second = (expert == ids[1:2, :]).astype(F32)
    s_row = lax.broadcasted_iota(jnp.int32, (ROWS, ROWS), 0)
    s_col = lax.broadcasted_iota(jnp.int32, (ROWS, ROWS), 1)
    earlier = ((s_row < s_col) & ((s_row >> 7) == (s_col >> 7))).astype(F32).astype(BF)
    seen = dot((first + second).astype(BF), earlier)
    rank_a = jnp.sum(first * seen, axis=0, keepdims=True)
    rank_b = jnp.sum(second * seen, axis=0, keepdims=True)
    owner = ids >> 2
    dy = ((owner >> 1) - y) & 3
    dc = (owner ^ c) & 1
    g = ((owner >> 3) - z - dy) & 3
    chunk_at = jnp.where(g == 0, (dy & 1) * 4, dc * 4 + g)
    k_at = jnp.where(g == 0, (dy >> 1) * 2 + dc, dy)
    block_at = lax.broadcasted_iota(jnp.int32, (2, ROWS), 1) >> 7
    rank = jnp.concatenate([rank_a, rank_b], axis=0)
    sent_at = chunk_at * CHUNK + (ids & 3) * 64 + k_at * 16 + block_at * CAP
    sent_at = jnp.where(
        chunk_at == 0, block_at * QUARTER + k_at * 16 + (ids & 3) * CAP, sent_at
    )
    back_at = chunk_at * QUARTER + k_at * 16 + (ids & 3) * CAP
    slots[0:2, :] = sent_at.astype(F32) + rank
    slots[2:4, :] = back_at.astype(F32) + rank

    p_row = lax.broadcasted_iota(jnp.int32, (CHUNK, CHUNK), 0)
    p_col = lax.broadcasted_iota(jnp.int32, (CHUNK, CHUNK), 1)
    p_from = ((p_row >> 2) & 3) * 64 + ((p_row >> 4) & 3) * 16 + (p_row >> 6) * 4 + (p_row & 3)
    turn[...] = (p_from == p_col).astype(F32).astype(BF)

    with jax.named_scope('wait_tokens'):
        loads[0].wait()
    for cp in loads[1:]:
        cp.start()

    def norm_step(i, carry):
        rows = pl.ds(pl.multiple_of(i * 64, 64), 64)
        wide = normed[rows, :].astype(F32)
        scale = lax.rsqrt(jnp.mean(wide * wide, axis=-1, keepdims=True) + EPS)
        normed[rows, :] = ((wide * scale) * gain_ref[...]).astype(BF)
        return carry

    with jax.named_scope('norm'):
        lax.fori_loop(0, ROWS // 64, norm_step, 0)

    def slot_rows(base, shape):
        return (lax.broadcasted_iota(jnp.int32, shape, 0) + base).astype(F32)

    def send_rows(i, k, rows):
        pltpu.make_async_remote_copy(
            src_ref=disp_send.at[i, rows], dst_ref=disp_recv.at[i, rows],
            send_sem=dsend.at[i], recv_sem=drecv.at[i],
            device_id=ep_peer(i, k), device_id_type=MESH_ID,
        ).start()

    def send_chunk(i):
        for j in range(LOCAL):
            for k in range(4):
                send_rows(i, k, pl.ds(j * 64 + k * 16, 16))

    def send_own_quarter():
        for n in range(N_TP):
            rows = pl.ds(n * QUARTER + 16, 16)
            pltpu.make_async_remote_copy(
                src_ref=disp_send.at[0, rows], dst_ref=disp_recv.at[0, rows],
                send_sem=gsend.at[4 + n], recv_sem=grecv.at[4 + n],
                device_id=ep_peer(0, 1), device_id_type=MESH_ID,
            ).start()
        for k in range(2, 4):
            send_rows(0, k, pl.ds(pl.multiple_of(x * QUARTER + k * 16, 16), 16))

    def wait_partner():
        for n in range(N_TP):
            rows = pl.ds(n * QUARTER + 16, 16)
            pltpu.make_async_remote_copy(
                src_ref=disp_send.at[0, rows], dst_ref=disp_recv.at[0, rows],
                send_sem=gsend.at[4 + n], recv_sem=grecv.at[4 + n],
                device_id=ep_peer(0, 1), device_id_type=MESH_ID,
            ).wait()

    def pass_on(which):
        halves = (slice(0, D // 2), slice(D // 2, D))

        def at(d, cols):
            first = lax.rem(x + d % N_TP, N_TP) * QUARTER + 32
            return disp_recv.at[0, pl.ds(pl.multiple_of(first, 32), 32), cols]

        routes = (
            (at(0, slice(0, D)), 1), (at(0, slice(0, D)), -1),
            (at(-1, halves[0]), 1), (at(1, halves[1]), -1),
        )
        return [
            pltpu.make_async_remote_copy(
                src_ref=routes[n][0], dst_ref=routes[n][0],
                send_sem=gsend.at[n], recv_sem=grecv.at[n],
                device_id=x_peer(routes[n][1]), device_id_type=MESH_ID,
            )
            for n in which
        ]

    def send_back(i):
        for k in range(4):
            rows = pl.ds(k * 16, 16)

            def start(rows=rows, k=k):
                pltpu.make_async_remote_copy(
                    src_ref=ret_send.at[i, rows], dst_ref=ret_recv.at[i, rows],
                    send_sem=tsend.at[i], recv_sem=trecv.at[i],
                    device_id=ep_peer(i, k, -1), device_id_type=MESH_ID,
                ).start()

            if k:
                start()
            else:
                pl.when(i > 0)(start)

    def wait_rows(buf, to, i, send_sem, recv_sem, count):
        rows = pl.ds(0, count)
        pltpu.make_async_remote_copy(
            src_ref=buf.at[i, rows], dst_ref=to.at[i, rows],
            send_sem=send_sem.at[i], recv_sem=recv_sem.at[i],
            device_id=ep_peer(0, 1), device_id_type=MESH_ID,
        ).wait()

    def wait_chunk(i, count):
        wait_rows(disp_send, disp_recv, i, dsend, drecv, count)

    def wait_back(i):
        pl.when(i == 0)(lambda: wait_rows(ret_send, ret_recv, i, tsend, trecv, QUARTER - 16))
        pl.when(i > 0)(lambda: wait_rows(ret_send, ret_recv, i, tsend, trecv, QUARTER))

    nxt = lax.rem(me + 1, N_EP)
    nxt_dev = (nxt // (NY * NC), lax.rem(nxt // NC, NY), lax.rem(nxt, NC), x)
    halos = [
        pltpu.make_async_remote_copy(
            src_ref=ref.at[pl.ds(ROWS - BLOCK, BLOCK)], dst_ref=halo.at[i],
            send_sem=hsend.at[i], recv_sem=hrecv.at[i],
            device_id=nxt_dev, device_id_type=MESH_ID,
        )
        for i, ref in enumerate((k_ref, v_ref))
    ]

    def gather_step(i, carry):
        index = slot_rows(i * CHUNK, (CHUNK, ROWS))
        pick = (index == slots[0:1, :]) | (index == slots[1:2, :])
        pick = pick.astype(F32).astype(BF)
        for n in range(N_TP):
            cols = slice(n * COLS, (n + 1) * COLS)
            disp_send[i, :, cols] = dot(pick, normed[:, cols]).astype(BF)

        if carry is None:
            with jax.named_scope('barrier'):
                pl.semaphore_wait(barrier, N_EP - 1 + N_TP - 1)
            for cp in halos:
                cp.start()
            send_own_quarter()
        else:
            send_chunk(i)
        return carry

    gather_step(0, None)
    lax.fori_loop(1, 2, gather_step, 0)
    for n in range(N_TP):
        rows = slice(n * QUARTER, n * QUARTER + 16)
        disp_recv[0, rows, :] = disp_send[0, rows, :]

    def x_copy(t, n, src, dst, d):
        return pltpu.make_async_remote_copy(
            src_ref=src, dst_ref=dst, send_sem=xsend.at[t, n], recv_sem=xrecv.at[t, n],
            device_id=x_peer(d), device_id_type=MESH_ID,
        )

    def x_copies(which, t, part, relay, sides):
        routes = (
            (part(2, 0), relay(0), 1),
            (part(2, 1), relay(1), -1),
            (part(1, 1), sides(0, 1), 1),
            (part(-1, 0), sides(1, 0), -1),
            (part(1, 0), sides(0, 0), 1),
            (part(-1, 1), sides(1, 1), -1),
        )
        return [x_copy(t, n, *routes[n]) for n in which]

    def start_first(*refs):
        for cp in x_copies((0, 1, 2, 3), *refs):
            cp.start()

    def start_second(t, part, relay, sides):
        for cp in x_copies((0, 1), t, part, relay, sides):
            cp.wait()
        for n, d in ((0, 1), (1, -1)):
            own = part(d, n)
            own[...] = (own[...].astype(F32) + relay(n)[...].astype(F32)).astype(BF)
        for cp in x_copies((4, 5), t, part, relay, sides):
            cp.start()

    def wait_rest(*refs):
        for cp in x_copies((2, 3, 4, 5), *refs):
            cp.wait()

    def summed(t, part, relay, sides, half):
        return (
            part(0, half)[...].astype(F32)
            + sides(0, half)[...].astype(F32) + sides(1, half)[...].astype(F32)
        )

    def by_quarter(t, buf, rows_in, relay, side):
        half = rows_in // 2

        def part(d, n):
            at = lax.rem(x + d % N_TP, N_TP) * rows_in + n * half
            return buf.at[pl.ds(pl.multiple_of(at, half), half)]

        return (
            t, part, lambda n: relay.at[n],
            lambda s, n: side.at[s, pl.ds(n * half, half)],
        )

    def shared_refs():
        return by_quarter(CHUNKS, sh_send, BLOCK, sh_relay, sh_side)

    def mixer_refs():
        return by_quarter(CHUNKS + 1, mix_send, BLOCK, mix_relay, mix_side)

    def expert_refs(i):
        return by_quarter(i, disp_send.at[i], QUARTER, rs_relay.at[i], rs_side.at[i])

    for cp in loads[1:4]:
        cp.wait()
    gate = dot(normed[...], sg[...])
    up = dot(normed[...], su[...])
    hidden = (gate / (1.0 + jnp.exp(-gate)) * up).astype(BF)
    for n in range(N_TP):
        cols = slice(n * COLS, (n + 1) * COLS)
        sh_send[:, cols] = dot(hidden, sd[:, cols]).astype(BF)

    for cp in x_copies((2, 3), *shared_refs()):
        cp.start()
    with jax.named_scope('own_quarter'):
        wait_chunk(0, 32)
    for cp in pass_on((0, 1)):
        cp.start()
    with jax.named_scope('gather'):
        lax.fori_loop(2, CHUNKS, gather_step, 0)
    with jax.named_scope('pass_on'):
        for cp in pass_on((0, 1)):
            cp.wait()
    for cp in pass_on((2, 3)):
        cp.start()
    for cp in x_copies((0, 1), *shared_refs()):
        cp.start()

    lane = lax.broadcasted_iota(jnp.int32, (1, 128), 1)
    low = lane < HEAD_DIM
    half_a = lax.broadcasted_iota(jnp.int32, (128, 128), 0) >> 6
    half_b = lax.broadcasted_iota(jnp.int32, (128, 128), 1) >> 6
    same_half = (half_a == half_b).astype(F32).astype(BF)

    q_gain = jnp.concatenate([qg_ref[...], qg_ref[...]], axis=1)
    k_gain = jnp.concatenate([kg_ref[...], kg_ref[...]], axis=1)

    def head_norm(rows_in, gain):
        wide = rows_in.astype(F32)
        square = wide * wide
        top = square.astype(BF)
        rest = (square - top.astype(F32)).astype(BF)
        total = dot(top, same_half) + dot(rest, same_half)
        scale = lax.rsqrt(total * (1.0 / HEAD_DIM) + EPS)
        return ((wide * scale) * gain).astype(BF)

    def both_halves(rows_in, dst, rows):
        wide = rows_in.astype(F32)
        turned = pltpu.roll(wide, HEAD_DIM, 1)
        dst[0, rows, :] = jnp.where(low, wide, turned).astype(BF)
        dst[1, rows, :] = jnp.where(low, turned, wide).astype(BF)

    own_rows = slice(BLOCK, BLOCK + ROWS)
    both_halves(head_norm(k_ref[...], k_gain), kd, own_rows)
    both_halves(v_ref[...], vd, own_rows)
    with jax.named_scope('halo_wait'):
        for cp in halos:
            cp.wait()
    both_halves(head_norm(halo[0], k_gain), kd, slice(0, BLOCK))
    both_halves(halo[1], vd, slice(0, BLOCK))
    query_pos = lax.broadcasted_iota(jnp.int32, (BLOCK, 2 * BLOCK), 0)
    key_pos = lax.broadcasted_iota(jnp.int32, (BLOCK, 2 * BLOCK), 1)

    def attend(n, carry):
        rows = pl.ds(pl.multiple_of(n * BLOCK, BLOCK), BLOCK)
        band = pl.ds(pl.multiple_of(n * BLOCK, BLOCK), 2 * BLOCK)
        floor = jnp.where(me * 4 + n == 0, BLOCK, 0)
        inside = (key_pos <= query_pos + BLOCK) & (key_pos > query_pos) & (key_pos >= floor)
        for kv in range(2):
            parts = []
            for b in range(2):
                cols = slice((kv * 2 + b) * 128, (kv * 2 + b + 1) * 128)
                qn = head_norm(q_ref[rows, cols], q_gain).astype(F32)
                parts.append(jnp.where(low, qn, 0.0).astype(BF))
                parts.append(jnp.where(low, 0.0, qn).astype(BF))
            stacked = jnp.concatenate(parts, axis=0)
            scores = lax.dot_general(
                stacked, kd[kv, band, :], (((1,), (1,)), ((), ())), preferred_element_type=F32
            ) * 0.125
            probs = []
            for g in range(4):
                sink = sink_ref[0, kv * 4 + g]
                part = jnp.where(inside, scores[g * BLOCK:(g + 1) * BLOCK], MASKED)
                top = jnp.maximum(jnp.max(part, axis=-1, keepdims=True), sink)
                ex = jnp.exp(part - top)
                den = jnp.sum(ex, axis=-1, keepdims=True) + jnp.exp(sink - top)
                probs.append((ex * (1.0 / den)).astype(BF))
            mixed = dot(jnp.concatenate(probs, axis=0), vd[kv, band, :])
            for b in range(2):
                lo = mixed[(2 * b) * BLOCK:(2 * b + 1) * BLOCK]
                hi = mixed[(2 * b + 1) * BLOCK:(2 * b + 2) * BLOCK]
                cols = slice((kv * 2 + b) * 128, (kv * 2 + b + 1) * 128)
                heads[rows, cols] = jnp.where(low, lo, hi).astype(BF)
        return carry

    with jax.named_scope('attend'):
        lax.fori_loop(0, ROWS // BLOCK, attend, 0)
    loads[4].wait()
    for n in range(N_TP):
        cols = slice(n * COLS, (n + 1) * COLS)
        mix_send[:, cols] = dot(heads[...], ow[:, cols]).astype(BF)

    start_first(*mixer_refs())
    with jax.named_scope('shared2'):
        start_second(*shared_refs())

    loads[5].wait()
    loads[6].wait()
    loads[7].wait()

    own_tokens = pl.ds(pl.multiple_of(x * BLOCK, BLOCK), BLOCK)

    def combine(i, carry):
        with jax.named_scope('wait_ret'):
            wait_back(i)
        with jax.named_scope('combine'):
            index = slot_rows(i * QUARTER, (QUARTER, BLOCK))
            weight = jnp.where(index == slots[2:3, own_tokens], rw_ref[0:1, own_tokens], 0.0)
            weight += jnp.where(index == slots[3:4, own_tokens], rw_ref[1:2, own_tokens], 0.0)
            main = weight.astype(BF)
            rest = (weight - main.astype(F32)).astype(BF)
            dims = (((0,), (0,)), ((), ()))
            acc[...] += lax.dot_general(
                main, ret_recv[i], dims, preferred_element_type=F32
            ) + lax.dot_general(rest, ret_recv[i], dims, preferred_element_type=F32)
        return carry

    def step(i, carry):
        @pl.when(i < CHUNKS)
        def _():
            with jax.named_scope('wait_disp'):
                pl.when(i > 0)(lambda: wait_chunk(i, CHUNK))

                @pl.when(i == 0)
                def _():
                    for cp in pass_on((2, 3)):
                        cp.wait()
                    wait_partner()
                    for n in range(N_TP):
                        cols = slice(n * COLS, (n + 1) * COLS)
                        disp_recv[0, :, cols] = dot(turn[...], disp_recv[0, :, cols]).astype(BF)

            with jax.named_scope('ffn'):
                wide = []
                for j in range(LOCAL):
                    came = disp_recv[i, j * 64:(j + 1) * 64, :]
                    gate = dot(came, wg[j])
                    up = dot(came, wu[j])
                    hidden = (gate / (1.0 + jnp.exp(-gate)) * up).astype(BF)
                    wide.append(dot(turn[:, j * 64:(j + 1) * 64], hidden).astype(BF))
                wide = jnp.concatenate(wide, axis=1)
                for n in range(N_TP):
                    cols = slice(n * COLS, (n + 1) * COLS)
                    disp_send[i, :, cols] = dot(wide, wd[:, cols]).astype(BF)

        @pl.when(i == 2)
        def _():
            with jax.named_scope('mix2'):
                start_second(*mixer_refs())

        @pl.when((i >= 1) & (i <= CHUNKS))
        def _():
            with jax.named_scope('rs2'):
                start_second(*expert_refs(i - 1))

        @pl.when(i < CHUNKS)
        def _():
            start_first(*expert_refs(i))

        @pl.when(i == CHUNKS)
        def _():
            with jax.named_scope('mix_out'):
                wait_rest(*mixer_refs())
                for half in range(2):
                    rows = slice(half * BLOCK // 2, (half + 1) * BLOCK // 2)
                    mix_out[rows, :] = summed(*mixer_refs(), half).astype(BF)

        @pl.when((i >= 2) & (i <= CHUNKS + 1))
        def _():
            h = i - 2
            with jax.named_scope('wait_rs'):
                wait_rest(*expert_refs(h))
            with jax.named_scope('ret'):
                for half in range(2):
                    rows = slice(half * QUARTER // 2, (half + 1) * QUARTER // 2)
                    ret_send[h, rows, :] = summed(*expert_refs(h), half).astype(BF)
                send_back(h)

            @pl.when(h == 0)
            def _():
                ret_recv[0, 0:16, :] = ret_send[0, 0:16, :]

        @pl.when(i == 3)
        def _():
            with jax.named_scope('wait_shared'):
                wait_rest(*shared_refs())
            for half in range(2):
                rows = slice(half * BLOCK // 2, (half + 1) * BLOCK // 2)
                acc[rows, :] = summed(*shared_refs(), half).astype(BF).astype(F32)

        first_h = jnp.where(i <= CHUNKS, 0, jnp.where(i == CHUNKS + 1, 3, 7))
        last_h = jnp.where(i < CHUNKS, 0, jnp.where(i == CHUNKS, 3, jnp.where(i == CHUNKS + 1, 7, 8)))
        lax.fori_loop(first_h, last_h, combine, 0)
        return carry

    lax.fori_loop(0, CHUNKS + 3, step, 0)
    exp_out[...] = acc[...].astype(BF)


def hand_over(mix_in, exp_in, mix_out, exp_out):
    mix_out[...] = mix_in[...]
    exp_out[...] = exp_in[...]


def shards(
    query_rows, key_rows, value_rows, query_gain, key_gain, sink_logit, out_weight, tokens,
    norm_gain, expert_ids, route_weight, gate_weight, up_weight, down_weight,
    shared_gate, shared_up, shared_down,
):
    vmem = pl.BlockSpec(memory_space=pltpu.VMEM)
    hbm = pl.BlockSpec(memory_space=pl.ANY)
    smem = pl.BlockSpec(memory_space=pltpu.SMEM)
    dma = pltpu.SemaphoreType.DMA
    out = jax.ShapeDtypeStruct((BLOCK, D), BF)
    results = pl.pallas_call(
        layer_kernel,
        out_shape=(out, out),
        in_specs=[vmem] * 5 + [smem] + [vmem] * 3 + [hbm] * 8,
        out_specs=(vmem, vmem),
        scratch_shapes=[
            pltpu.VMEM((ROWS, D), BF),
            pltpu.VMEM((ROWS, D), BF),
            pltpu.VMEM((LOCAL, D, FFS), BF),
            pltpu.VMEM((LOCAL, D, FFS), BF),
            pltpu.VMEM((LOCAL * FFS, D), BF),
            pltpu.VMEM((D, FFS), BF),
            pltpu.VMEM((D, FFS), BF),
            pltpu.VMEM((FFS, D), BF),
            pltpu.VMEM((4, ROWS), F32),
            pltpu.VMEM((CHUNKS, CHUNK, D), BF),
            pltpu.VMEM((CHUNKS, CHUNK, D), BF),
            pltpu.VMEM((CHUNKS, 2, QUARTER // 2, D), BF),
            pltpu.VMEM((CHUNKS, 2, QUARTER, D), BF),
            pltpu.VMEM((CHUNKS, QUARTER, D), BF),
            pltpu.VMEM((CHUNKS, QUARTER, D), BF),
            pltpu.VMEM((ROWS, D), BF),
            pltpu.VMEM((2, BLOCK // 2, D), BF),
            pltpu.VMEM((2, BLOCK, D), BF),
            pltpu.VMEM((ROWS, D), BF),
            pltpu.VMEM((2, BLOCK // 2, D), BF),
            pltpu.VMEM((2, BLOCK, D), BF),
            pltpu.VMEM((BLOCK, D), F32),
            pltpu.VMEM((CHUNK, CHUNK), BF),
            pltpu.VMEM((2, BLOCK, 128), BF),
            pltpu.VMEM((2, BLOCK + ROWS, 128), BF),
            pltpu.VMEM((2, BLOCK + ROWS, 128), BF),
            pltpu.VMEM((ROWS, 512), BF),
            dma((8,)),
            dma((CHUNKS,)), dma((CHUNKS,)),
            dma((8,)), dma((8,)),
            dma((CHUNKS + 2, 6)), dma((CHUNKS + 2, 6)),
            dma((CHUNKS,)), dma((CHUNKS,)),
            dma((2,)), dma((2,)),
        ],
        compiler_params=pltpu.CompilerParams(
            collective_id=0, has_side_effects=True, vmem_limit_bytes=67000000
        ),
        name="layer",
    )(
        query_rows, key_rows, value_rows,
        query_gain[None], key_gain[None],
        sink_logit[None], norm_gain[None], expert_ids.T, route_weight.T,
        tokens, out_weight, gate_weight, up_weight, down_weight.reshape(LOCAL * FFS, D),
        shared_gate, shared_up, shared_down,
    )
    return tuple(
        pl.pallas_call(
            hand_over, out_shape=(out, out), in_specs=[vmem] * 2, out_specs=(vmem, vmem),
            name="hand_over",
        )(*results)
    )


def solution(mesh):
    split = Mesh(mesh.devices.reshape(NZ, NY, NC, mesh.shape["tp"]), EP_TP)
    return jax.shard_map(
        shards,
        mesh=split,
        in_specs=(
            P(EP, "x"), P(EP, "x"), P(EP, "x"), P(), P(), P("x"), P("x", None),
            P(EP, None), P(), P(EP, None), P(EP, None),
            P(EP, None, "x"), P(EP, None, "x"), P(EP, "x", None),
            P(None, "x"), P(None, "x"), P("x", None),
        ),
        out_specs=(P(EP_TP, None), P(EP_TP, None)),
        check_vma=False,
    )
```

```python
import jax
import jax.numpy as jnp
from jax import lax
from jax.experimental import pallas as pl
from jax.experimental.pallas import tpu as pltpu
from jax.sharding import Mesh
from jax.sharding import PartitionSpec as P

HEADS = 32
KV_HEADS = 8
HEAD_DIM = 64
BLOCK = 128
CAP = 4
N_TP = 4
NZ, NY, NC = 4, 4, 2
N_EP = NZ * NY * NC
EP = ("z", "y", "c")
EP_TP = ("z", "y", "c", "x")
D = 2048
ROWS = 512
FFS = 256
EXPERTS = 128
LOCAL = 4
COLS = D // N_TP
EPS = 1e-06
MASKED = -1e30
MESH_ID = pl.DeviceIdType.MESH
BF = jnp.bfloat16
F32 = jnp.float32

CHUNKS = N_EP // 4
CHUNK = 4 * LOCAL * 16
QUARTER = CHUNK // N_TP


def dot(a, b):
    return jnp.dot(a, b, preferred_element_type=F32)


def layer_kernel(
    q_ref, k_ref, v_ref, qg_ref, kg_ref, sink_ref, gain_ref, ids_ref, rw_ref,
    tok_hbm, ow_hbm, wg_hbm, wu_hbm, wd_hbm, sg_hbm, su_hbm, sd_hbm,
    mix_out, exp_out,
    normed, ow, wg, wu, wd, sg, su, sd,
    slots, disp_send, disp_recv, rs_relay, rs_side, ret_send, ret_recv,
    mix_send, mix_relay, mix_side, sh_send, sh_relay, sh_side, acc, turn,
    halo, kd, vd, heads,
    load_sem, dsend, drecv, gsend, grecv, xsend, xrecv, tsend, trecv, hsend, hrecv,
):
    z, y, c, x = (lax.axis_index(a) for a in EP_TP)
    me = (z * NY + y) * NC + c

    def ep_peer(chunk, k, sign=1):
        g, dc = lax.rem(chunk, 4), chunk // 4
        latin = (g + 3) // 4
        both = 2 * (k // 2) + dc
        dy = latin * k + (1 - latin) * both
        dz = latin * lax.rem(g + k, 4) + (1 - latin) * both
        dc = latin * dc + (1 - latin) * (k % 2)
        if sign < 0:
            dy, dz = NY - dy, NZ - dz
        return (lax.rem(z + dz, NZ), lax.rem(y + dy, NY), lax.rem(c + dc, NC), x)

    def x_peer(d):
        return (z, y, c, lax.rem(x + d % N_TP, N_TP))

    barrier = pltpu.get_barrier_semaphore()
    for owner in range(1, N_EP):
        pl.semaphore_signal(
            barrier, inc=1, device_id=ep_peer(owner // 4, owner % 4), device_id_type=MESH_ID
        )
    for d in range(1, N_TP):
        pl.semaphore_signal(barrier, inc=1, device_id=x_peer(d), device_id_type=MESH_ID)

    loads = [
        pltpu.make_async_copy(s, t, load_sem.at[i])
        for i, (s, t) in enumerate(
            [(tok_hbm, normed), (sg_hbm, sg), (su_hbm, su), (sd_hbm, sd), (ow_hbm, ow),
             (wg_hbm, wg), (wu_hbm, wu), (wd_hbm, wd)]
        )
    ]
    loads[0].start()

    ids = ids_ref[...]
    expert = lax.broadcasted_iota(jnp.int32, (EXPERTS, ROWS), 0)
    first = (expert == ids[0:1, :]).astype(F32)
    second = (expert == ids[1:2, :]).astype(F32)
    s_row = lax.broadcasted_iota(jnp.int32, (ROWS, ROWS), 0)
    s_col = lax.broadcasted_iota(jnp.int32, (ROWS, ROWS), 1)
    earlier = ((s_row < s_col) & ((s_row >> 7) == (s_col >> 7))).astype(F32).astype(BF)
    seen = dot((first + second).astype(BF), earlier)
    rank_a = jnp.sum(first * seen, axis=0, keepdims=True)
    rank_b = jnp.sum(second * seen, axis=0, keepdims=True)
    owner = ids >> 2
    dy = ((owner >> 1) - y) & 3
    dc = (owner ^ c) & 1
    g = ((owner >> 3) - z - dy) & 3
    chunk_at = jnp.where(g == 0, (dy & 1) * 4, dc * 4 + g)
    k_at = jnp.where(g == 0, (dy >> 1) * 2 + dc, dy)
    block_at = lax.broadcasted_iota(jnp.int32, (2, ROWS), 1) >> 7
    rank = jnp.concatenate([rank_a, rank_b], axis=0)
    sent_at = chunk_at * CHUNK + (ids & 3) * 64 + k_at * 16 + block_at * CAP
    sent_at = jnp.where(
        chunk_at == 0, block_at * QUARTER + k_at * 16 + (ids & 3) * CAP, sent_at
    )
    back_at = chunk_at * QUARTER + k_at * 16 + (ids & 3) * CAP
    slots[0:2, :] = sent_at.astype(F32) + rank
    slots[2:4, :] = back_at.astype(F32) + rank

    p_row = lax.broadcasted_iota(jnp.int32, (CHUNK, CHUNK), 0)
    p_col = lax.broadcasted_iota(jnp.int32, (CHUNK, CHUNK), 1)
    p_from = ((p_row >> 2) & 3) * 64 + ((p_row >> 4) & 3) * 16 + (p_row >> 6) * 4 + (p_row & 3)
    turn[...] = (p_from == p_col).astype(F32).astype(BF)

    with jax.named_scope('wait_tokens'):
        loads[0].wait()
    for cp in loads[1:]:
        cp.start()

    def norm_step(i, carry):
        rows = pl.ds(pl.multiple_of(i * 64, 64), 64)
        wide = normed[rows, :].astype(F32)
        scale = lax.rsqrt(jnp.mean(wide * wide, axis=-1, keepdims=True) + EPS)
        normed[rows, :] = ((wide * scale) * gain_ref[...]).astype(BF)
        return carry

    with jax.named_scope('norm'):
        lax.fori_loop(0, ROWS // 64, norm_step, 0)

    def slot_rows(base, shape):
        return (lax.broadcasted_iota(jnp.int32, shape, 0) + base).astype(F32)

    def send_rows(i, k, rows):
        pltpu.make_async_remote_copy(
            src_ref=disp_send.at[i, rows], dst_ref=disp_recv.at[i, rows],
            send_sem=dsend.at[i], recv_sem=drecv.at[i],
            device_id=ep_peer(i, k), device_id_type=MESH_ID,
        ).start()

    def send_chunk(i):
        for j in range(LOCAL):
            for k in range(4):
                send_rows(i, k, pl.ds(j * 64 + k * 16, 16))

    def send_own_quarter():
        for n in range(N_TP):
            rows = pl.ds(n * QUARTER + 16, 16)
            pltpu.make_async_remote_copy(
                src_ref=disp_send.at[0, rows], dst_ref=disp_recv.at[0, rows],
                send_sem=gsend.at[4 + n], recv_sem=grecv.at[4 + n],
                device_id=ep_peer(0, 1), device_id_type=MESH_ID,
            ).start()
        for k in range(2, 4):
            send_rows(0, k, pl.ds(pl.multiple_of(x * QUARTER + k * 16, 16), 16))

    def wait_partner():
        for n in range(N_TP):
            rows = pl.ds(n * QUARTER + 16, 16)
            pltpu.make_async_remote_copy(
                src_ref=disp_send.at[0, rows], dst_ref=disp_recv.at[0, rows],
                send_sem=gsend.at[4 + n], recv_sem=grecv.at[4 + n],
                device_id=ep_peer(0, 1), device_id_type=MESH_ID,
            ).wait()

    def pass_on(which):
        halves = (slice(0, D // 2), slice(D // 2, D))

        def at(d, cols):
            first = lax.rem(x + d % N_TP, N_TP) * QUARTER + 32
            return disp_recv.at[0, pl.ds(pl.multiple_of(first, 32), 32), cols]

        routes = (
            (at(0, slice(0, D)), 1), (at(0, slice(0, D)), -1),
            (at(-1, halves[0]), 1), (at(1, halves[1]), -1),
        )
        return [
            pltpu.make_async_remote_copy(
                src_ref=routes[n][0], dst_ref=routes[n][0],
                send_sem=gsend.at[n], recv_sem=grecv.at[n],
                device_id=x_peer(routes[n][1]), device_id_type=MESH_ID,
            )
            for n in which
        ]

    def send_back(i):
        for k in range(4):
            rows = pl.ds(k * 16, 16)

            def start(rows=rows, k=k):
                pltpu.make_async_remote_copy(
                    src_ref=ret_send.at[i, rows], dst_ref=ret_recv.at[i, rows],
                    send_sem=tsend.at[i], recv_sem=trecv.at[i],
                    device_id=ep_peer(i, k, -1), device_id_type=MESH_ID,
                ).start()

            if k:
                start()
            else:
                pl.when(i > 0)(start)

    def wait_rows(buf, to, i, send_sem, recv_sem, count):
        rows = pl.ds(0, count)
        pltpu.make_async_remote_copy(
            src_ref=buf.at[i, rows], dst_ref=to.at[i, rows],
            send_sem=send_sem.at[i], recv_sem=recv_sem.at[i],
            device_id=ep_peer(0, 1), device_id_type=MESH_ID,
        ).wait()

    def wait_chunk(i, count):
        wait_rows(disp_send, disp_recv, i, dsend, drecv, count)

    def wait_back(i):
        pl.when(i == 0)(lambda: wait_rows(ret_send, ret_recv, i, tsend, trecv, QUARTER - 16))
        pl.when(i > 0)(lambda: wait_rows(ret_send, ret_recv, i, tsend, trecv, QUARTER))

    nxt = lax.rem(me + 1, N_EP)
    nxt_dev = (nxt // (NY * NC), lax.rem(nxt // NC, NY), lax.rem(nxt, NC), x)
    halos = [
        pltpu.make_async_remote_copy(
            src_ref=ref.at[pl.ds(ROWS - BLOCK, BLOCK)], dst_ref=halo.at[i],
            send_sem=hsend.at[i], recv_sem=hrecv.at[i],
            device_id=nxt_dev, device_id_type=MESH_ID,
        )
        for i, ref in enumerate((k_ref, v_ref))
    ]

    def gather_step(i, carry):
        index = slot_rows(i * CHUNK, (CHUNK, ROWS))
        pick = (index == slots[0:1, :]) | (index == slots[1:2, :])
        pick = pick.astype(F32).astype(BF)
        for n in range(N_TP):
            cols = slice(n * COLS, (n + 1) * COLS)
            disp_send[i, :, cols] = dot(pick, normed[:, cols]).astype(BF)

        if carry is None:
            with jax.named_scope('barrier'):
                pl.semaphore_wait(barrier, N_EP - 1 + N_TP - 1)
            for cp in halos:
                cp.start()
            send_own_quarter()
        else:
            send_chunk(i)
        return carry

    gather_step(0, None)
    lax.fori_loop(1, 2, gather_step, 0)
    for n in range(N_TP):
        rows = slice(n * QUARTER, n * QUARTER + 16)
        disp_recv[0, rows, :] = disp_send[0, rows, :]

    def x_copy(t, n, src, dst, d):
        return pltpu.make_async_remote_copy(
            src_ref=src, dst_ref=dst, send_sem=xsend.at[t, n], recv_sem=xrecv.at[t, n],
            device_id=x_peer(d), device_id_type=MESH_ID,
        )

    def x_copies(which, t, part, relay, sides):
        routes = (
            (part(2, 0), relay(0), 1),
            (part(2, 1), relay(1), -1),
            (part(1, 1), sides(0, 1), 1),
            (part(-1, 0), sides(1, 0), -1),
            (part(1, 0), sides(0, 0), 1),
            (part(-1, 1), sides(1, 1), -1),
        )
        return [x_copy(t, n, *routes[n]) for n in which]

    def start_first(*refs):
        for cp in x_copies((0, 1, 2, 3), *refs):
            cp.start()

    def start_second(t, part, relay, sides):
        for cp in x_copies((0, 1), t, part, relay, sides):
            cp.wait()
        for n, d in ((0, 1), (1, -1)):
            own = part(d, n)
            own[...] = (own[...].astype(F32) + relay(n)[...].astype(F32)).astype(BF)
        for cp in x_copies((4, 5), t, part, relay, sides):
            cp.start()

    def wait_rest(*refs):
        for cp in x_copies((2, 3, 4, 5), *refs):
            cp.wait()

    def summed(t, part, relay, sides, half):
        return (
            part(0, half)[...].astype(F32)
            + sides(0, half)[...].astype(F32) + sides(1, half)[...].astype(F32)
        )

    def by_quarter(t, buf, rows_in, relay, side):
        half = rows_in // 2

        def part(d, n):
            at = lax.rem(x + d % N_TP, N_TP) * rows_in + n * half
            return buf.at[pl.ds(pl.multiple_of(at, half), half)]

        return (
            t, part, lambda n: relay.at[n],
            lambda s, n: side.at[s, pl.ds(n * half, half)],
        )

    def shared_refs():
        return by_quarter(CHUNKS, sh_send, BLOCK, sh_relay, sh_side)

    def mixer_refs():
        return by_quarter(CHUNKS + 1, mix_send, BLOCK, mix_relay, mix_side)

    def expert_refs(i):
        return by_quarter(i, disp_send.at[i], QUARTER, rs_relay.at[i], rs_side.at[i])

    for cp in loads[1:4]:
        cp.wait()
    gate = dot(normed[...], sg[...])
    up = dot(normed[...], su[...])
    hidden = (gate / (1.0 + jnp.exp(-gate)) * up).astype(BF)
    for n in range(N_TP):
        cols = slice(n * COLS, (n + 1) * COLS)
        sh_send[:, cols] = dot(hidden, sd[:, cols]).astype(BF)

    for cp in x_copies((2, 3), *shared_refs()):
        cp.start()
    lane = lax.broadcasted_iota(jnp.int32, (1, 128), 1)
    low = lane < HEAD_DIM
    half_a = lax.broadcasted_iota(jnp.int32, (128, 128), 0) >> 6
    half_b = lax.broadcasted_iota(jnp.int32, (128, 128), 1) >> 6
    same_half = (half_a == half_b).astype(F32).astype(BF)

    q_gain = jnp.concatenate([qg_ref[...], qg_ref[...]], axis=1)
    k_gain = jnp.concatenate([kg_ref[...], kg_ref[...]], axis=1)

    def head_norm(rows_in, gain):
        wide = rows_in.astype(F32)
        square = wide * wide
        top = square.astype(BF)
        rest = (square - top.astype(F32)).astype(BF)
        total = dot(top, same_half) + dot(rest, same_half)
        scale = lax.rsqrt(total * (1.0 / HEAD_DIM) + EPS)
        return ((wide * scale) * gain).astype(BF)

    def both_halves(rows_in, dst, rows):
        wide = rows_in.astype(F32)
        turned = pltpu.roll(wide, HEAD_DIM, 1)
        dst[0, rows, :] = jnp.where(low, wide, turned).astype(BF)
        dst[1, rows, :] = jnp.where(low, turned, wide).astype(BF)

    own_rows = slice(BLOCK, BLOCK + ROWS)
    both_halves(head_norm(k_ref[...], k_gain), kd, own_rows)
    both_halves(v_ref[...], vd, own_rows)
    with jax.named_scope('halo_wait'):
        for cp in halos:
            cp.wait()
    both_halves(head_norm(halo[0], k_gain), kd, slice(0, BLOCK))
    both_halves(halo[1], vd, slice(0, BLOCK))
    query_pos = lax.broadcasted_iota(jnp.int32, (BLOCK, 2 * BLOCK), 0)
    key_pos = lax.broadcasted_iota(jnp.int32, (BLOCK, 2 * BLOCK), 1)

    def attend(n, carry):
        rows = pl.ds(pl.multiple_of(n * BLOCK, BLOCK), BLOCK)
        band = pl.ds(pl.multiple_of(n * BLOCK, BLOCK), 2 * BLOCK)
        floor = jnp.where(me * 4 + n == 0, BLOCK, 0)
        inside = (key_pos <= query_pos + BLOCK) & (key_pos > query_pos) & (key_pos >= floor)
        for kv in range(2):
            parts = []
            for b in range(2):
                cols = slice((kv * 2 + b) * 128, (kv * 2 + b + 1) * 128)
                qn = head_norm(q_ref[rows, cols], q_gain).astype(F32)
                parts.append(jnp.where(low, qn, 0.0).astype(BF))
                parts.append(jnp.where(low, 0.0, qn).astype(BF))
            stacked = jnp.concatenate(parts, axis=0)
            scores = lax.dot_general(
                stacked, kd[kv, band, :], (((1,), (1,)), ((), ())), preferred_element_type=F32
            ) * 0.125
            probs = []
            for g in range(4):
                sink = sink_ref[0, kv * 4 + g]
                part = jnp.where(inside, scores[g * BLOCK:(g + 1) * BLOCK], MASKED)
                top = jnp.maximum(jnp.max(part, axis=-1, keepdims=True), sink)
                ex = jnp.exp(part - top)
                den = jnp.sum(ex, axis=-1, keepdims=True) + jnp.exp(sink - top)
                probs.append((ex * (1.0 / den)).astype(BF))
            mixed = dot(jnp.concatenate(probs, axis=0), vd[kv, band, :])
            for b in range(2):
                lo = mixed[(2 * b) * BLOCK:(2 * b + 1) * BLOCK]
                hi = mixed[(2 * b + 1) * BLOCK:(2 * b + 2) * BLOCK]
                cols = slice((kv * 2 + b) * 128, (kv * 2 + b + 1) * 128)
                heads[rows, cols] = jnp.where(low, lo, hi).astype(BF)
        return carry

    with jax.named_scope('attend'):
        lax.fori_loop(0, ROWS // BLOCK, attend, 0)
    with jax.named_scope('own_quarter'):
        wait_chunk(0, 32)
    for cp in pass_on((0, 1)):
        cp.start()
    with jax.named_scope('gather'):
        lax.fori_loop(2, CHUNKS, gather_step, 0)
    with jax.named_scope('pass_on'):
        for cp in pass_on((0, 1)):
            cp.wait()
    for cp in pass_on((2, 3)):
        cp.start()
    for cp in x_copies((0, 1), *shared_refs()):
        cp.start()

    loads[4].wait()
    for n in range(N_TP):
        cols = slice(n * COLS, (n + 1) * COLS)
        mix_send[:, cols] = dot(heads[...], ow[:, cols]).astype(BF)

    start_first(*mixer_refs())
    with jax.named_scope('shared2'):
        start_second(*shared_refs())

    loads[5].wait()
    loads[6].wait()
    loads[7].wait()

    own_tokens = pl.ds(pl.multiple_of(x * BLOCK, BLOCK), BLOCK)

    def combine(i, carry):
        with jax.named_scope('wait_ret'):
            wait_back(i)
        with jax.named_scope('combine'):
            index = slot_rows(i * QUARTER, (QUARTER, BLOCK))
            weight = jnp.where(index == slots[2:3, own_tokens], rw_ref[0:1, own_tokens], 0.0)
            weight += jnp.where(index == slots[3:4, own_tokens], rw_ref[1:2, own_tokens], 0.0)
            main = weight.astype(BF)
            rest = (weight - main.astype(F32)).astype(BF)
            dims = (((0,), (0,)), ((), ()))
            acc[...] += lax.dot_general(
                main, ret_recv[i], dims, preferred_element_type=F32
            ) + lax.dot_general(rest, ret_recv[i], dims, preferred_element_type=F32)
        return carry

    def step(i, carry):
        @pl.when(i < CHUNKS)
        def _():
            with jax.named_scope('wait_disp'):
                pl.when(i > 0)(lambda: wait_chunk(i, CHUNK))

                @pl.when(i == 0)
                def _():
                    for cp in pass_on((2, 3)):
                        cp.wait()
                    wait_partner()
                    for n in range(N_TP):
                        cols = slice(n * COLS, (n + 1) * COLS)
                        disp_recv[0, :, cols] = dot(turn[...], disp_recv[0, :, cols]).astype(BF)

            with jax.named_scope('ffn'):
                wide = []
                for j in range(LOCAL):
                    came = disp_recv[i, j * 64:(j + 1) * 64, :]
                    gate = dot(came, wg[j])
                    up = dot(came, wu[j])
                    hidden = (gate / (1.0 + jnp.exp(-gate)) * up).astype(BF)
                    wide.append(dot(turn[:, j * 64:(j + 1) * 64], hidden).astype(BF))
                wide = jnp.concatenate(wide, axis=1)
                for n in range(N_TP):
                    cols = slice(n * COLS, (n + 1) * COLS)
                    disp_send[i, :, cols] = dot(wide, wd[:, cols]).astype(BF)

        @pl.when(i == 2)
        def _():
            with jax.named_scope('mix2'):
                start_second(*mixer_refs())

        @pl.when((i >= 1) & (i <= CHUNKS))
        def _():
            with jax.named_scope('rs2'):
                start_second(*expert_refs(i - 1))

        @pl.when(i < CHUNKS)
        def _():
            start_first(*expert_refs(i))

        @pl.when((i >= 2) & (i <= CHUNKS + 1))
        def _():
            h = i - 2
            with jax.named_scope('wait_rs'):
                wait_rest(*expert_refs(h))
            with jax.named_scope('ret'):
                for half in range(2):
                    rows = slice(half * QUARTER // 2, (half + 1) * QUARTER // 2)
                    ret_send[h, rows, :] = summed(*expert_refs(h), half).astype(BF)
                send_back(h)

            @pl.when(h == 0)
            def _():
                ret_recv[0, 0:16, :] = ret_send[0, 0:16, :]

        @pl.when(i == 3)
        def _():
            with jax.named_scope('wait_shared'):
                wait_rest(*shared_refs())
            for half in range(2):
                rows = slice(half * BLOCK // 2, (half + 1) * BLOCK // 2)
                acc[rows, :] = summed(*shared_refs(), half).astype(BF).astype(F32)

        @pl.when(i == CHUNKS + 1)
        def _():
            with jax.named_scope('mix_out'):
                wait_rest(*mixer_refs())
                for half in range(2):
                    rows = slice(half * BLOCK // 2, (half + 1) * BLOCK // 2)
                    mix_out[rows, :] = summed(*mixer_refs(), half).astype(BF)

        first_h = jnp.where(i <= CHUNKS + 1, 0, 7)
        last_h = jnp.where(i < CHUNKS + 1, 0, jnp.where(i == CHUNKS + 1, 7, 8))
        lax.fori_loop(first_h, last_h, combine, 0)
        return carry

    lax.fori_loop(0, CHUNKS + 3, step, 0)
    exp_out[...] = acc[...].astype(BF)


def hand_over(mix_in, exp_in, mix_out, exp_out, held, in_sem, out_sem):
    pairs = [(src, dst, n) for n in range(2) for src, dst in ((mix_in, mix_out), (exp_in, exp_out))]
    half = BLOCK // 2
    copies_in, copies_out = [], []
    for at, (src, dst, n) in enumerate(pairs):
        rows = pl.ds(n * half, half)
        copies_in.append(pltpu.make_async_copy(src.at[rows], held.at[at], in_sem.at[at]))
        copies_out.append(pltpu.make_async_copy(held.at[at], dst.at[rows], out_sem.at[at]))
    for cp in copies_in:
        cp.start()
    for got, put in zip(copies_in, copies_out):
        got.wait()
        put.start()
    for cp in copies_out:
        cp.wait()


def shards(
    query_rows, key_rows, value_rows, query_gain, key_gain, sink_logit, out_weight, tokens,
    norm_gain, expert_ids, route_weight, gate_weight, up_weight, down_weight,
    shared_gate, shared_up, shared_down,
):
    vmem = pl.BlockSpec(memory_space=pltpu.VMEM)
    hbm = pl.BlockSpec(memory_space=pl.ANY)
    smem = pl.BlockSpec(memory_space=pltpu.SMEM)
    dma = pltpu.SemaphoreType.DMA
    out = jax.ShapeDtypeStruct((BLOCK, D), BF)
    results = pl.pallas_call(
        layer_kernel,
        out_shape=(out, out),
        in_specs=[vmem] * 5 + [smem] + [vmem] * 3 + [hbm] * 8,
        out_specs=(vmem, vmem),
        scratch_shapes=[
            pltpu.VMEM((ROWS, D), BF),
            pltpu.VMEM((ROWS, D), BF),
            pltpu.VMEM((LOCAL, D, FFS), BF),
            pltpu.VMEM((LOCAL, D, FFS), BF),
            pltpu.VMEM((LOCAL * FFS, D), BF),
            pltpu.VMEM((D, FFS), BF),
            pltpu.VMEM((D, FFS), BF),
            pltpu.VMEM((FFS, D), BF),
            pltpu.VMEM((4, ROWS), F32),
            pltpu.VMEM((CHUNKS, CHUNK, D), BF),
            pltpu.VMEM((CHUNKS, CHUNK, D), BF),
            pltpu.VMEM((CHUNKS, 2, QUARTER // 2, D), BF),
            pltpu.VMEM((CHUNKS, 2, QUARTER, D), BF),
            pltpu.VMEM((CHUNKS, QUARTER, D), BF),
            pltpu.VMEM((CHUNKS, QUARTER, D), BF),
            pltpu.VMEM((ROWS, D), BF),
            pltpu.VMEM((2, BLOCK // 2, D), BF),
            pltpu.VMEM((2, BLOCK, D), BF),
            pltpu.VMEM((ROWS, D), BF),
            pltpu.VMEM((2, BLOCK // 2, D), BF),
            pltpu.VMEM((2, BLOCK, D), BF),
            pltpu.VMEM((BLOCK, D), F32),
            pltpu.VMEM((CHUNK, CHUNK), BF),
            pltpu.VMEM((2, BLOCK, 128), BF),
            pltpu.VMEM((2, BLOCK + ROWS, 128), BF),
            pltpu.VMEM((2, BLOCK + ROWS, 128), BF),
            pltpu.VMEM((ROWS, 512), BF),
            dma((8,)),
            dma((CHUNKS,)), dma((CHUNKS,)),
            dma((8,)), dma((8,)),
            dma((CHUNKS + 2, 6)), dma((CHUNKS + 2, 6)),
            dma((CHUNKS,)), dma((CHUNKS,)),
            dma((2,)), dma((2,)),
        ],
        compiler_params=pltpu.CompilerParams(
            collective_id=0, has_side_effects=True, vmem_limit_bytes=67000000
        ),
        name="layer",
    )(
        query_rows, key_rows, value_rows,
        query_gain[None], key_gain[None],
        sink_logit[None], norm_gain[None], expert_ids.T, route_weight.T,
        tokens, out_weight, gate_weight, up_weight, down_weight.reshape(LOCAL * FFS, D),
        shared_gate, shared_up, shared_down,
    )
    return tuple(
        pl.pallas_call(
            hand_over, out_shape=(out, out), in_specs=[hbm] * 2, out_specs=(hbm, hbm),
            scratch_shapes=[pltpu.VMEM((4, BLOCK // 2, D), BF), dma((4,)), dma((4,))],
            name="hand_over",
        )(*results)
    )


def solution(mesh):
    split = Mesh(mesh.devices.reshape(NZ, NY, NC, mesh.shape["tp"]), EP_TP)
    return jax.shard_map(
        shards,
        mesh=split,
        in_specs=(
            P(EP, "x"), P(EP, "x"), P(EP, "x"), P(), P(), P("x"), P("x", None),
            P(EP, None), P(), P(EP, None), P(EP, None),
            P(EP, None, "x"), P(EP, None, "x"), P(EP, "x", None),
            P(None, "x"), P(None, "x"), P("x", None),
        ),
        out_specs=(P(EP_TP, None), P(EP_TP, None)),
        check_vma=False,
    )
```
